32 devices in a mesh: grp: 2 (over y), ep: 16 (over z, x, core), tp: 1.
Axes of the slice: x: 2, y: 2, z: 4, core: 2. Of those that a mesh axis runs over, the one named last changes fastest.
Arguments:
- tokens: bfloat16 [3072, 2048], P(('grp', 'ep')), parts along dimension 0, may hold values from -6 to 6
- prior_state: float32 [2, 3072, 4096], P(None, ('grp', 'ep'), 'tp'), parts along dimension 1, may hold values from -6 to 6
- mix_gain: float32 [2048], replicated, may hold values from 0.1 to 1.9
- in_weight: bfloat16 [2048, 1024], P(None, 'tp'), may hold values from -0.125 to 0.125
- decay_rate: float32 [64, 64], P('tp'), may hold values from 0.2 to 20
- frequency: float32 [64, 64], P('tp'), may hold values from 0 to 12
- log_step: float32 [64], P('tp'), may hold values from -4.6 to 0
- input_map: float32 [2, 64, 64, 16], P(None, 'tp'), may hold values from -6 to 6
- output_map: float32 [2, 64, 16, 64], P(None, 'tp'), may hold values from -0.5 to 0.5
- skip_gain: float32 [1024], P('tp'), may hold values from -4 to 4
- out_weight: bfloat16 [1024, 2048], P('tp'), may hold values from -0.1875 to 0.1875
- channel_gain: float32 [2048], replicated, may hold values from 0.1 to 1.9
- expert_gate: bfloat16 [16, 2048, 512], P('ep', None, 'tp'), may hold values from -0.125 to 0.125
- expert_up: bfloat16 [16, 2048, 512], P('ep', None, 'tp'), may hold values from -0.125 to 0.125
- expert_down: bfloat16 [16, 512, 2048], P('ep', 'tp'), may hold values from -0.25 to 0.25
- shared_gate: bfloat16 [2048, 512], P(None, 'tp'), may hold values from -0.125 to 0.125
- shared_up: bfloat16 [2048, 512], P(None, 'tp'), may hold values from -0.125 to 0.125
- shared_down: bfloat16 [512, 2048], P('tp'), may hold values from -0.25 to 0.25
- routes: int32 [3072, 6], P(('grp', 'ep')), parts along dimension 0, may hold values from 0 to 15, all different within a row; in each aligned block of 96 rows (0 to 95, 96 to 191, ...) at most 54 rows name the same one
- route_weights: float32 [3072, 6], P(('grp', 'ep')), parts along dimension 0, may hold values from 0.05 to 0.8
Outputs:
- layer_out: bfloat16 [3072, 2048], P(('grp', 'ep'), 'tp'), parts along dimension 0
- new_state: float32 [2, 3072, 4096], P(None, ('grp', 'ep'), 'tp'), parts along dimension 1
The draws below stay inside these ranges and needn't reach their ends.
There are 2 independent parts, one for each index of `grp`. The reference program is written for one: setup_inputs(seed, part) draws one part's arguments, and reference() takes and returns one part's arrays. A program takes and returns all parts, laid end to end along the dimension named above; an argument that names none is the same for every part. Nothing has to cross between parts.
Inputs may be any that keep to these rules, and one draw needn't show every extreme that they name: `routes`: each row names 6 different experts; among the rows of one index of ep no expert is named by more than 54 rows.
All inputs are finite; a program needn't handle non-finite values.
Results may differ from the reference program's by a relative error of at most 0.017.
Values may be sent and summed in bfloat16 or wider, within the bound.
A program may use at most 128 MiB of HBM per device.

```python
import math
import jax
import jax.numpy as jnp
import numpy as np
from jax import lax

D = 2048
SSM_WIDTH = 1024
GROUPS = 64
GROUP_WIDTH = 16
STATE = 64
EXP_WIDTH = 512
SHARED_WIDTH = 512
TOPK = 6
SEQ_DEV = 96
SEQS = 1536
EXPERTS = 16
CAP = 54
N_EP = 16
N_TP = 1


def block_levels(stream_key, extent, pieces, smallest, high):
    def one(position, blocks):
        heights = jax.random.uniform(jax.random.fold_in(jax.random.fold_in(stream_key, 6), position), (blocks,), jnp.float32, smallest / len(pieces), high / len(pieces))
        return jnp.repeat(jnp.exp(heights), extent[position] // blocks).reshape((-1,) + (1,) * (len(extent) - position - 1))

    factor_of = one(*pieces[0])
    for cut in pieces[1:]:
        factor_of = factor_of * one(*cut)
    return factor_of


def deal_out(rng, own, number, rows, number_of, top, reach, skew):
    order = jax.random.permutation(rng, number_of)
    packed, ordinary = shares(number_of, rows * top, reach, skew, True), shares(number_of, rows * top, reach, skew, False)
    places = jnp.arange(number_of)

    def named(sizes, offset_by):
        used = int((sizes > 0).sum())
        fixed = max(1, used // 4)
        passed = fixed + (places - fixed + offset_by * (used - fixed)) % max(1, number_of - fixed)
        return jnp.zeros((number_of,), jnp.int32).at[order[jnp.where(places < fixed, places, passed)]].set(jnp.asarray(sizes, jnp.int32))

    sizes = jnp.where(number % 4 == 0, named(packed, number // 4), named(ordinary, number - number // 4 - 1))
    mixed = jax.random.permutation(jax.random.fold_in(own, 3), number_of)
    donor, receiver = mixed[0:number_of // 2 * 2:2], mixed[1:number_of // 2 * 2:2]
    margin = jnp.minimum(sizes[donor] - 1, reach - sizes[receiver]) // 2
    margin = jnp.where((donor == order[0]) | (receiver == order[0]) | (sizes[receiver] == 0), 0, jnp.maximum(margin, 0))
    passed = jax.random.randint(jax.random.fold_in(own, 4), (number_of // 2,), 0, 1 << 20) % (margin + 1)
    sizes = sizes.at[donor].add(-passed).at[receiver].add(passed)
    labels = jnp.searchsorted(jnp.cumsum(sizes), jnp.arange(rows * top), side="right").astype(jnp.int32)
    grid = labels.reshape(top, rows).T
    grid = grid[jax.random.permutation(jax.random.fold_in(own, 1), rows)]
    offset_by = jax.random.randint(jax.random.fold_in(own, 2), (rows, 1), 0, top)
    return jnp.take_along_axis(grid, (jnp.arange(top)[None, :] + offset_by) % top, axis=1)


def shares(amount, total, reach, slope, full):
    weights = [(1 << 20) // math.isqrt(rank ** slope) + 1 for rank in range(1, amount + 1)]
    largest = reach if full else min(reach, max(-(-total // amount), total * weights[0] // sum(weights)))
    least = 1 if total - largest >= amount - 1 else 0
    counts, spare = [largest] + [least] * (amount - 1), total - largest - least * (amount - 1)
    while spare > 0:
        free = [i for i in range(1, amount) if counts[i] < largest] or [i for i in range(1, amount) if counts[i] < reach]
        mass, left = sum([weights[i] for i in free]), spare
        for i in free:
            more = min(reach - counts[i], max(1, left * weights[i] // mass), spare)
            counts[i] = counts[i] + more
            spare = spare - more
    return np.array(counts)


def gaussian(key, dims, spread, most, shards=(), held_as=jnp.bfloat16):
    drawn = spread * jax.random.normal(key, dims, jnp.float32)
    if shards:
        drawn = drawn * block_levels(key, dims, shards, -0.22, 0.18)
    return jnp.clip(drawn, -most, most).astype(held_as)


def setup_inputs(seed: int = 0, part: int = 0) -> dict:
    keys = jax.random.split(jax.random.key(seed), 21)
    part_keys = jax.random.split(jax.random.fold_in(keys[20], part), 21)
    tokens = gaussian(part_keys[0], (SEQS, D), 1.0, 6.0, ((0, 16),))
    prior_state = gaussian(part_keys[1], (2, SEQS, GROUPS * STATE), 1.0, 6.0, ((1, 16),), jnp.float32)
    mix_gain = jnp.clip(1.0 + 0.18 * jax.random.normal(keys[2], (D,), jnp.float32), 0.1, 1.9)
    in_weight = gaussian(keys[3], (D, SSM_WIDTH), D ** -0.5, 0.125)
    decay_rate = jnp.clip(jnp.exp(jax.random.uniform(keys[4], (GROUPS, STATE), jnp.float32, math.log(0.2), math.log(20.0))), 0.2, 20.0)
    frequency = jnp.clip(jax.random.uniform(keys[5], (GROUPS, STATE), jnp.float32, 0.0, 12.0), 0.0, 12.0)
    log_step = jnp.clip(jax.random.uniform(keys[6], (GROUPS,), jnp.float32, -4.6, 0.0), -4.6, 0.0)
    input_map = gaussian(keys[7], (2, GROUPS, STATE, GROUP_WIDTH), 1.0, 6.0, (), jnp.float32)
    output_map = gaussian(keys[8], (2, GROUPS, GROUP_WIDTH, STATE), (2 * STATE) ** -0.5, 0.5, (), jnp.float32)
    skip_gain = gaussian(keys[9], (SSM_WIDTH,), 1.0, 4.0, (), jnp.float32)
    out_weight = gaussian(keys[10], (SSM_WIDTH, D), SSM_WIDTH ** -0.5, 0.1875)
    channel_gain = jnp.clip(1.0 + 0.18 * jax.random.normal(keys[11], (D,), jnp.float32), 0.1, 1.9)
    expert_gate = gaussian(keys[12], (EXPERTS, D, EXP_WIDTH), D ** -0.5, 0.125, ((0, 16),))
    expert_up = gaussian(keys[13], (EXPERTS, D, EXP_WIDTH), D ** -0.5, 0.125, ((0, 16),))
    expert_down = gaussian(keys[14], (EXPERTS, EXP_WIDTH, D), EXP_WIDTH ** -0.5, 0.25, ((0, 16),))
    shared_gate = gaussian(keys[15], (D, SHARED_WIDTH), D ** -0.5, 0.125)
    shared_up = gaussian(keys[16], (D, SHARED_WIDTH), D ** -0.5, 0.125)
    shared_down = gaussian(keys[17], (SHARED_WIDTH, D), SHARED_WIDTH ** -0.5, 0.25)
    routes_keys = jax.random.split(jax.random.fold_in(part_keys[18], 1), SEQS // SEQ_DEV)
    routes_turns = jax.random.permutation(jax.random.fold_in(part_keys[18], 3), SEQS // SEQ_DEV)
    routes = jax.vmap(lambda own, number: deal_out(jax.random.fold_in(part_keys[18], 2), own, number, SEQ_DEV, EXPERTS, TOPK, CAP, 2))(routes_keys, routes_turns).reshape((SEQS, TOPK))
    route_weights = jnp.clip(0.05 + 0.75 * jax.random.uniform(part_keys[19], (SEQS, TOPK), jnp.float32) ** block_levels(part_keys[19], (SEQS, TOPK), ((0, 16),), -0.2, 0.2), 0.05, 0.8)
    return {"tokens": tokens, "prior_state": prior_state, "mix_gain": mix_gain, "in_weight": in_weight, "decay_rate": decay_rate, "frequency": frequency, "log_step": log_step, "input_map": input_map, "output_map": output_map, "skip_gain": skip_gain, "out_weight": out_weight, "channel_gain": channel_gain, "expert_gate": expert_gate, "expert_up": expert_up, "expert_down": expert_down, "shared_gate": shared_gate, "shared_up": shared_up, "shared_down": shared_down, "routes": routes, "route_weights": route_weights}


norm_eps = 1e-06
highest = lax.Precision.HIGHEST

def root_scale(activations, scale_gain):
    values = activations.astype(jnp.float32)
    factor = lax.rsqrt(lax.optimization_barrier(jnp.mean(values * values, axis=-1, keepdims=True)) + norm_eps)
    return (values * factor * scale_gain).astype(jnp.bfloat16)

def state_update(drive_rows, prior_state, decay_rate, frequency, log_step, input_map, output_map, skip_gain):
    sequences = drive_rows.shape[0]
    groups = decay_rate.shape[0]
    driven = drive_rows.astype(jnp.float32).reshape(sequences, groups, -1)
    step_size = jnp.exp(log_step)[:, None]
    real_rate = -decay_rate
    magnitude = jnp.exp(real_rate * step_size)
    turn_real = magnitude * jnp.cos(frequency * step_size)
    turn_imag = magnitude * jnp.sin(frequency * step_size)
    denominator = real_rate * real_rate + frequency * frequency
    hold_real = ((turn_real - 1.0) * real_rate + turn_imag * frequency) / denominator
    hold_imag = (turn_imag * real_rate - (turn_real - 1.0) * frequency) / denominator
    push_real = jnp.einsum('sgh,gph->sgp', driven, input_map[0], precision=highest)
    push_imag = jnp.einsum('sgh,gph->sgp', driven, input_map[1], precision=highest)
    enter_real = push_real * hold_real - push_imag * hold_imag
    enter_imag = push_real * hold_imag + push_imag * hold_real
    old_real = prior_state[0].reshape(sequences, groups, -1)
    old_imag = prior_state[1].reshape(sequences, groups, -1)
    fresh_real = turn_real * old_real - turn_imag * old_imag + enter_real
    fresh_imag = turn_real * old_imag + turn_imag * old_real + enter_imag
    readout = jnp.einsum('ghp,sgp->sgh', output_map[0], fresh_real, precision=highest)
    readout = readout - jnp.einsum('ghp,sgp->sgh', output_map[1], fresh_imag, precision=highest)
    readout = readout.reshape(sequences, -1) + skip_gain * drive_rows.astype(jnp.float32)
    fresh = jnp.stack([fresh_real.reshape(sequences, -1), fresh_imag.reshape(sequences, -1)])
    return (readout, fresh)

def split_block(activations, gate_weight, up_weight, down_weight):
    col_width = gate_weight.shape[1] // N_TP
    summed = jnp.zeros((activations.shape[0], down_weight.shape[1]), jnp.float32)
    for portion in range(N_TP):
        lower = portion * col_width
        gate_val = jnp.dot(activations, gate_weight[:, lower:lower + col_width], preferred_element_type=jnp.float32)
        up_val = jnp.dot(activations, up_weight[:, lower:lower + col_width], preferred_element_type=jnp.float32)
        hidden = (jax.nn.silu(gate_val) * up_val).astype(jnp.bfloat16)
        piece = jnp.dot(hidden, down_weight[lower:lower + col_width], preferred_element_type=jnp.float32)
        summed = summed + lax.optimization_barrier(piece.astype(jnp.bfloat16)).astype(jnp.float32)
    return summed

def reference(tokens, prior_state, mix_gain, in_weight, decay_rate, frequency, log_step, input_map, output_map, skip_gain, out_weight, channel_gain, expert_gate, expert_up, expert_down, shared_gate, shared_up, shared_down, routes, route_weights):
    normed = root_scale(tokens, mix_gain)
    drive_rows = jnp.dot(normed, in_weight, preferred_element_type=jnp.float32).astype(jnp.bfloat16)
    readout, new_state = state_update(drive_rows, prior_state, decay_rate, frequency, log_step, input_map, output_map, skip_gain)
    activated = jax.nn.gelu(readout).astype(jnp.bfloat16)
    col_width = out_weight.shape[0] // N_TP
    mixer_out = jnp.zeros((SEQS, D), jnp.float32)
    for portion in range(N_TP):
        lower = portion * col_width
        piece = jnp.dot(activated[:, lower:lower + col_width], out_weight[lower:lower + col_width], preferred_element_type=jnp.float32)
        mixer_out = mixer_out + lax.optimization_barrier(piece.astype(jnp.bfloat16)).astype(jnp.float32)
    middle = (tokens.astype(jnp.float32) + mixer_out).astype(jnp.bfloat16)
    second_normed = root_scale(middle, channel_gain)
    shared_out = split_block(second_normed, shared_gate, shared_up, shared_down)
    slot_limit = N_EP * CAP
    flat_routes = routes.reshape(-1)
    flat_weights = route_weights.reshape(-1)

    def one_expert(running, operands):
        expert_id, gate_weight, up_weight, down_weight = operands
        matched = flat_routes == expert_id
        chosen = jnp.nonzero(matched, size=slot_limit, fill_value=0)[0].astype(jnp.int32)
        found_count = jnp.sum(matched.astype(jnp.int32))
        is_valid = jnp.arange(slot_limit, dtype=jnp.int32) < found_count
        row_index = chosen // TOPK
        picked_rows = jnp.take(second_normed, row_index, axis=0)
        produced = split_block(picked_rows, gate_weight, up_weight, down_weight).astype(jnp.bfloat16)
        produced = lax.optimization_barrier(produced).astype(jnp.float32)
        weight_vals = jnp.where(is_valid, jnp.take(flat_weights, chosen), jnp.zeros_like(flat_weights[:1]))
        running = running.at[row_index].add(weight_vals[:, None] * produced)
        return (running, None)
    routed, _ = lax.scan(one_expert, jnp.zeros((SEQS, D), jnp.float32), (jnp.arange(EXPERTS, dtype=jnp.int32), expert_gate, expert_up, expert_down))
    layer_out = (middle.astype(jnp.float32) + routed + shared_out).astype(jnp.bfloat16)
    return (layer_out, new_state)
```

```python
import functools
import jax
import jax.numpy as jnp
from jax import lax
from jax.experimental import pallas as pl
from jax.experimental.pallas import tpu as pltpu
from jax.sharding import PartitionSpec as P

norm_eps = 1e-06
highest = lax.Precision.HIGHEST
MESH = pl.DeviceIdType.MESH


def root_scale(activations, scale_gain):
    values = activations.astype(jnp.float32)
    factor = lax.rsqrt(jnp.mean(values * values, axis=-1, keepdims=True) + norm_eps)
    return (values * factor * scale_gain).astype(jnp.bfloat16)


def state_update(
    drive_rows, prior_state, decay_rate, frequency, log_step, input_map, output_map, skip_gain
):
    sequences = drive_rows.shape[0]
    groups = decay_rate.shape[0]
    driven = drive_rows.astype(jnp.float32).reshape(sequences, groups, -1)
    step_size = jnp.exp(log_step)[:, None]
    real_rate = -decay_rate
    magnitude = jnp.exp(real_rate * step_size)
    turn_real = magnitude * jnp.cos(frequency * step_size)
    turn_imag = magnitude * jnp.sin(frequency * step_size)
    denominator = real_rate * real_rate + frequency * frequency
    hold_real = ((turn_real - 1.0) * real_rate + turn_imag * frequency) / denominator
    hold_imag = (turn_imag * real_rate - (turn_real - 1.0) * frequency) / denominator
    push_real = jnp.einsum("sgh,gph->sgp", driven, input_map[0], precision=highest)
    push_imag = jnp.einsum("sgh,gph->sgp", driven, input_map[1], precision=highest)
    enter_real = push_real * hold_real - push_imag * hold_imag
    enter_imag = push_real * hold_imag + push_imag * hold_real
    old_real = prior_state[0].reshape(sequences, groups, -1)
    old_imag = prior_state[1].reshape(sequences, groups, -1)
    fresh_real = turn_real * old_real - turn_imag * old_imag + enter_real
    fresh_imag = turn_real * old_imag + turn_imag * old_real + enter_imag
    readout = jnp.einsum("ghp,sgp->sgh", output_map[0], fresh_real, precision=highest)
    readout = readout - jnp.einsum("ghp,sgp->sgh", output_map[1], fresh_imag, precision=highest)
    readout = readout.reshape(sequences, -1) + skip_gain * drive_rows.astype(jnp.float32)
    fresh = jnp.stack([fresh_real.reshape(sequences, -1), fresh_imag.reshape(sequences, -1)])
    return (readout, fresh)


def exchanged_experts(second_normed, routes, route_weights, expert_gate, expert_up, expert_down):
    experts = lax.axis_size("ep")
    seq_rows, top_count = routes.shape
    slot_cap = min(seq_rows, max(2, 3 * seq_rows * top_count // (2 * experts)))
    flat_routes = routes.reshape(-1)
    one_hot = (flat_routes[:, None] == jnp.arange(experts, dtype=jnp.int32)[None, :]).astype(
        jnp.int32
    )
    ranked = jnp.sum((jnp.cumsum(one_hot, axis=0) - one_hot) * one_hot, axis=1)
    slot_index = flat_routes * slot_cap + ranked
    placed = slot_index[:, None] == jnp.arange(experts * slot_cap, dtype=jnp.int32)[None, :]
    placed_rows = jnp.any(placed.reshape(seq_rows, top_count, experts * slot_cap), axis=1).astype(
        jnp.bfloat16
    )
    outgoing = lax.dot_general(
        placed_rows, second_normed, (((0,), (0,)), ((), ())), preferred_element_type=jnp.float32
    ).astype(jnp.bfloat16)
    outgoing = outgoing.reshape(experts, slot_cap, -1)
    arrived = lax.all_to_all(outgoing, "ep", split_axis=0, concat_axis=0, tiled=True)
    sources, count_items, full_width = arrived.shape
    expert_rows = arrived.reshape(sources * count_items, full_width)
    gate_val = jnp.dot(expert_rows, expert_gate[0], preferred_element_type=jnp.float32)
    up_val = jnp.dot(expert_rows, expert_up[0], preferred_element_type=jnp.float32)
    hidden = (jax.nn.silu(gate_val) * up_val).astype(jnp.bfloat16)
    piece = jnp.dot(hidden, expert_down[0], preferred_element_type=jnp.float32)
    summed = lax.psum_scatter(
        piece.reshape(sources, count_items, full_width).astype(jnp.bfloat16),
        "tp",
        scatter_dimension=2,
        tiled=True,
    )
    returned = lax.all_to_all(summed, "ep", split_axis=0, concat_axis=0, tiled=True)
    flat_back = returned.reshape(experts * slot_cap, -1)
    picked = (
        jnp.take(flat_back, slot_index, axis=0).reshape(seq_rows, top_count, -1).astype(jnp.float32)
    )
    routed = jnp.einsum("sk,skd->sd", route_weights, picked)
    return routed


PIECES = (
    (1, 0, 1, 0, 8),
    (0, 1, 1, 0, 8),
    (1, 2, 1, 0, 8),
    (0, 3, 1, 0, 8),
    (0, 4, 1, 0, 8),
    (0, 5, 1, 0, 5),
    (1, 5, 1, 5, 3),
)

END_PROGRAM = (
    (0, 0, 0, 0, 2), (0, 0, 0, 0, 0), (0, 0, 0, 1, 2), (0, 0, 0, 1, 0), (0, 0, 0, 3, 2),
    (0, 0, 0, 2, 2), (0, 0, 0, 3, 0), (5,), (0, 0, 1, 0, 0), (0, 0, 0, 2, 0), (0, 0, 0, 4, 0),
    (0, 1, 0, 1, 2), (0, 1, 0, 3, 2), (0, 0, 0, 4, 2), (0, 0, 1, 2, 0), (0, 0, 0, 5, 0),
    (0, 0, 0, 6, 0), (3, ((0, (0,)),)), (0, 2, 0, 1, 2), (0, 0, 0, 5, 2), (0, 0, 0, 6, 2),
    (3, ((1, (0,)),)), (4, ((0, (0,)),)), (1, 0, 1, 1, 2), (4, ((1, (0,)),)), (1, 1, 0, 0, 0),
    (1, 1, 1, 0, 0), (0, 3, 0, 1, 2), (1, 1, 1, 1, 2), (0, 0, 1, 6, 0), (3, ((2, (0,)),)),
    (4, ((2, (0,)),)), (1, 2, 0, 0, 0), (1, 2, 1, 0, 0), (1, 2, 1, 1, 2), (0, 3, 0, 3, 2),
    (3, ((3, (0,)),)), (0, 2, 0, 3, 2), (4, ((3, (0,)),)), (1, 3, 0, 0, 0), (1, 3, 1, 0, 0),
    (1, 3, 1, 1, 2), (1, 2, 0, 1, 0), (1, 1, 0, 1, 0), (3, ((2, (1,)), (3, (1,)))),
    (1, 3, 0, 1, 0), (4, ((2, (1,)), (3, (1,)))), (0, 3, 0, 4, 2), (1, 3, 0, 2, 0),
    (1, 3, 1, 2, 0), (1, 3, 1, 3, 2), (1, 2, 0, 2, 0), (1, 2, 1, 2, 0), (1, 2, 1, 3, 2),
    (0, 3, 0, 5, 2), (3, ((1, (1,)),)), (4, ((1, (1,)),)), (0, 2, 0, 4, 2), (1, 3, 0, 3, 0),
    (1, 1, 1, 3, 2), (0, 2, 0, 5, 2), (1, 2, 0, 3, 0), (1, 1, 0, 2, 0), (1, 1, 1, 2, 0),
    (0, 1, 0, 4, 2), (0, 1, 0, 5, 2), (3, ((0, (1,)), (3, (2,)))), (4, ((0, (1,)), (3, (2,)))),
    (1, 3, 0, 6, 0), (1, 3, 1, 4, 2), (1, 3, 1, 5, 2), (1, 3, 1, 6, 0), (1, 1, 0, 3, 0),
    (3, ((2, (2,)),)), (4, ((2, (2,)),)), (1, 2, 0, 6, 0), (1, 2, 1, 4, 2), (1, 2, 1, 5, 2),
    (1, 0, 1, 0, 2), (3, ((0, (2,)), (1, (2,)))), (1, 3, 0, 4, 0), (4, ((0, (2,)), (1, (2,)))),
    (1, 3, 0, 5, 0), (1, 2, 1, 6, 0), (1, 1, 1, 4, 2), (1, 1, 1, 5, 2), (2, 0, 0, 1),
    (1, 2, 0, 4, 0), (1, 2, 0, 5, 0), (1, 1, 0, 6, 0), (1, 1, 1, 6, 0), (1, 0, 1, 2, 2),
    (1, 0, 1, 3, 2), (2, 0, 0, 0), (1, 1, 0, 4, 0), (1, 1, 0, 5, 0), (1, 0, 1, 6, 2),
    (1, 0, 1, 4, 2), (1, 0, 1, 5, 2), (2, 0, 0, 2), (2, 0, 0, 3), (2, 0, 0, 6), (2, 0, 0, 4),
    (2, 0, 0, 5),
)

MID_PROGRAM = (
    (0, 1, 0, 0, 2), (0, 1, 0, 0, 0), (0, 1, 0, 0, 1), (0, 1, 0, 1, 2), (0, 1, 0, 1, 0),
    (0, 1, 0, 1, 1), (0, 1, 0, 3, 2), (0, 1, 0, 2, 2), (0, 1, 0, 3, 0), (0, 1, 0, 3, 1), (5,),
    (0, 0, 0, 0, 0), (0, 2, 0, 0, 1), (0, 0, 0, 1, 2), (0, 0, 0, 1, 0), (0, 1, 1, 0, 0),
    (0, 2, 0, 1, 2), (0, 2, 0, 1, 1), (0, 1, 1, 0, 1), (0, 0, 0, 3, 2), (0, 0, 1, 0, 0),
    (0, 0, 0, 3, 0), (0, 3, 0, 0, 1), (3, ((1, (0,)),)), (0, 0, 0, 2, 0), (0, 3, 0, 1, 2),
    (0, 2, 0, 3, 2), (0, 3, 0, 1, 1), (0, 2, 1, 0, 1), (4, ((1, (0,)),)), (1, 1, 1, 1, 2),
    (0, 0, 1, 2, 0), (0, 1, 0, 2, 0), (0, 1, 1, 2, 0), (0, 0, 0, 4, 0), (0, 3, 1, 0, 1),
    (0, 0, 0, 5, 0), (0, 1, 0, 4, 0), (0, 1, 0, 5, 0), (0, 0, 0, 6, 0), (0, 3, 0, 3, 2),
    (0, 0, 0, 4, 2), (0, 0, 0, 5, 2), (0, 1, 0, 4, 2), (0, 1, 0, 5, 2), (0, 1, 0, 6, 2),
    (0, 3, 0, 3, 1), (0, 2, 0, 3, 1), (0, 3, 0, 2, 1), (0, 3, 1, 2, 1), (0, 2, 0, 2, 1),
    (0, 2, 1, 2, 1), (0, 0, 1, 6, 0), (0, 1, 0, 6, 0), (0, 3, 0, 4, 2), (0, 3, 0, 4, 1),
    (0, 3, 0, 5, 2), (0, 3, 0, 5, 1), (0, 1, 0, 2, 1), (0, 1, 1, 2, 1), (0, 2, 0, 4, 2),
    (0, 2, 0, 4, 1), (0, 1, 1, 6, 0), (3, ((0, (1,)), (1, (1, 2)), (2, (0,)))), (0, 2, 0, 5, 2),
    (0, 2, 0, 5, 1), (0, 1, 0, 4, 1), (0, 1, 0, 5, 1), (0, 3, 0, 6, 1), (0, 3, 1, 6, 1),
    (0, 2, 0, 6, 1), (4, ((0, (1,)), (1, (1, 2)), (2, (0,)))), (0, 2, 1, 6, 1), (1, 0, 1, 3, 2),
    (1, 2, 0, 0, 0), (1, 2, 1, 0, 0), (1, 2, 1, 1, 2), (1, 1, 1, 3, 2),
    (3, ((0, (0,)), (3, (0, 2)))), (4, ((0, (0,)), (3, (0, 2)))), (1, 3, 0, 0, 0),
    (1, 3, 1, 0, 0), (1, 3, 1, 1, 2), (1, 3, 1, 4, 2), (3, ((0, (2,)), (2, (1, 2)), (3, (1,)))),
    (1, 2, 0, 1, 0), (4, ((0, (2,)), (2, (1, 2)), (3, (1,)))), (1, 3, 0, 2, 0), (1, 3, 1, 3, 2),
    (1, 3, 1, 5, 2), (1, 0, 1, 1, 2), (1, 0, 0, 0, 1), (1, 2, 1, 3, 2), (1, 1, 1, 0, 2),
    (1, 2, 1, 4, 2), (1, 2, 1, 5, 2), (1, 0, 1, 4, 2), (1, 0, 1, 5, 2), (1, 3, 0, 1, 0),
    (1, 3, 1, 2, 0), (1, 0, 1, 0, 1), (0, 1, 0, 6, 1), (0, 1, 1, 6, 1), (2, 1, 0, 1),
    (1, 3, 0, 3, 0), (1, 2, 0, 2, 0), (1, 2, 1, 2, 0), (1, 0, 0, 2, 1), (1, 0, 0, 1, 1),
    (1, 0, 1, 2, 1), (1, 3, 0, 6, 0), (1, 0, 0, 3, 1), (1, 3, 1, 6, 0), (1, 2, 0, 3, 0),
    (2, 1, 0, 0), (1, 2, 0, 6, 0), (1, 1, 1, 2, 2), (1, 1, 1, 4, 2), (1, 1, 1, 5, 2),
    (1, 0, 0, 6, 1), (1, 3, 0, 4, 0), (1, 0, 1, 6, 1), (1, 3, 0, 5, 0), (1, 2, 1, 6, 0),
    (2, 1, 0, 3), (1, 2, 0, 4, 0), (2, 1, 0, 2), (1, 2, 0, 5, 0), (1, 0, 0, 4, 1),
    (1, 0, 0, 5, 1), (1, 1, 1, 6, 2), (2, 1, 0, 4), (2, 1, 0, 6), (2, 1, 0, 5),
)

PLAN = ((END_PROGRAM, MID_PROGRAM), PIECES)


def plane_kernel(
    plan, tiles,
    own, middle, weights, gate_in, up_in, down_in, sgate_in, sup_in, sdown_in,
    out,
    rows_all, partial, from_level, from_side, table, scale,
    gate, up, down, sgate, sup, sdown, hidden, shared,
    load_sem, twin_send, twin_recv, w_send, w_recv,
    row_recv, level_recv, side_recv, send_sem,
):
    programs, pieces = plan
    experts = lax.axis_size("ep")
    me = lax.axis_index("ep")
    core = lax.rem(me, 2)
    node = me // 2
    col = lax.rem(node, 2)
    level = node // 2
    nodes = experts // 2
    top = nodes // 2 - 1
    rows, width = own.shape
    tile = rows // tiles
    hid = sgate.shape[1]
    flipped = level * 2 > top
    upward = jnp.where(flipped, -1, 1)
    twin = node * 2 + 1 - core

    def to_level(q):
        return jnp.where(flipped, top - q, q)

    def to_col(rel):
        return col if rel == 0 else 1 - col

    def to_node(q, rel):
        return to_level(q) * 2 + to_col(rel)

    def region(base, piece):
        at, high, left, wide = pieces[piece][1:]
        return (
            pl.ds(pl.multiple_of(base * rows + at * tile, tile), high * tile),
            pl.ds(left * width // 8, wide * width // 8),
        )

    loads = [
        pltpu.make_async_copy(src, dst, load_sem.at[n])
        for n, (src, dst) in enumerate(
            (
                (sgate_in, sgate), (sup_in, sup), (sdown_in, sdown),
                (gate_in.at[0], gate.at[core]), (up_in.at[0], up.at[core]),
                (down_in.at[0], down.at[pl.ds(pl.multiple_of(core * hid, hid), hid)]),
            )
        )
    ]
    for load in loads:
        load.start()

    barrier = pltpu.get_barrier_semaphore()
    for step in range(1, experts):
        pl.semaphore_signal(
            barrier, inc=1, device_id={"ep": lax.rem(me + step, experts)}, device_id_type=MESH
        )
    pl.semaphore_wait(barrier, experts - 1)

    def remote(src, dst, send, recv, target):
        return pltpu.make_async_remote_copy(
            src_ref=src, dst_ref=dst, send_sem=send, recv_sem=recv,
            device_id={"ep": target}, device_id_type=MESH,
        )

    always = []
    for step in range(1, nodes):
        other = lax.rem(node + step, nodes)
        copy = remote(
            weights.at[pl.ds(other * 2, 2)], table.at[node],
            w_send.at[step], w_recv.at[nodes - step], other * 2 + core,
        )
        copy.start()
        always.append(copy)
    twins = [
        remote(src, dst, twin_send.at[n], twin_recv.at[n], twin)
        for n, (src, dst) in enumerate(
            (
                (gate_in.at[0], gate.at[core]), (up_in.at[0], up.at[core]),
                (down_in.at[0], down.at[pl.ds(pl.multiple_of(core * hid, hid), hid)]),
            )
        )
    ]

    def twin_ready(n):
        refs = (gate.at[1 - core], up.at[1 - core],
                down.at[pl.ds(pl.multiple_of((1 - core) * hid, hid), hid)])
        remote(refs[n], refs[n], twin_send.at[n], twin_recv.at[n], twin).wait_recv()

    def strips(spot, first, others, store):
        row, lanes = spot
        wide = lanes.size
        step = 512 if wide % 512 == 0 else 256

        def strip(n, carry):
            at = pl.ds(pl.multiple_of(lanes.start + n * step, 128), step)
            value = first[row, at].astype(jnp.float32)
            for view in others:
                value = value + view(at).astype(jnp.float32)
            store(at, value)
            return carry

        lax.fori_loop(0, wide // step, strip, 0)

    def feed_in(base, source, take, gates, chunks, factor):
        def first(n, carry):
            data = source()
            gate_w, up_w = gates(n)
            g = jnp.dot(data, gate_w, preferred_element_type=jnp.float32)
            u = jnp.dot(data, up_w, preferred_element_type=jnp.float32)
            at = pl.ds(pl.multiple_of(n * 256, 256), 256)
            hidden[pl.ds(base, take), at] = factor(n, jax.nn.silu(g) * u).astype(jnp.bfloat16)
            return carry

        lax.fori_loop(0, chunks, first, 0)

    def feed_out(base, take, depth, down_w, finish):
        def second(n, carry):
            cols = pl.ds(pl.multiple_of(n * 512, 512), 512)
            piece = jnp.dot(
                hidden[pl.ds(base, take), pl.ds(0, depth)], down_w[:, cols],
                preferred_element_type=jnp.float32,
            )
            finish(cols, piece.astype(jnp.bfloat16))
            return carry

        lax.fori_loop(0, width // 512, second, 0)

    halves = hid // 256
    depths = hidden.shape[0] // (4 * rows)

    def shared_expert():
        for load in loads[:3]:
            load.wait()

        def gates(n):
            cols = pl.ds(pl.multiple_of(n * 256, 256), 256)
            return sgate[:, cols], sup[:, cols]

        feed_in(0, lambda: own[...], rows, gates, halves, lambda n, value: value)

        def keep(cols, piece):
            shared[:, cols] = piece

        feed_out(0, rows, hid, sdown, keep)

    def spread_table():
        for step in range(1, nodes):
            other = lax.rem(node + step, nodes)
            remote(
                table.at[other], table.at[other], w_send.at[step], w_recv.at[step], twin
            ).wait_recv()
        table[node] = weights[pl.ds(node * 2, 2)]

        def one(n, carry):
            for e in range(2):
                line = jnp.broadcast_to(table[n, e], (128, 128))
                scale[e, pl.ds(pl.multiple_of(n * rows, tile), rows), :] = jnp.transpose(line)[:rows]
            return carry

        lax.fori_loop(0, nodes, one, 0)

    def run(program, position):
        sends = []
        landed = set()
        dealt = set()
        held = {}

        def push(src, dst, recv, target):
            copy = remote(src, dst, send_sem.at[len(sends)], recv, target)
            copy.start()
            sends.append(copy)

        def row_in(q, rel, piece):
            if (q, rel) == (position, 0) or (q, rel, piece) in landed:
                return
            landed.add((q, rel, piece))
            origin = to_node(q, rel)
            view = rows_all.at[region(origin, piece)]
            remote(view, view, send_sem.at[0], row_recv.at[origin, piece], twin).wait_recv()

        def neighbour(way):
            if way == 2:
                return level * 2 + 1 - col
            return (level + (upward if way == 0 else -upward)) * 2 + col

        def pass_row(q, rel, piece, way):
            row_in(q, rel, piece)
            origin = to_node(q, rel)
            if (q, rel) == (position, 0):
                src = own.at[region(0, piece)]
            else:
                src = rows_all.at[region(origin, piece)]
            push(
                src, rows_all.at[region(origin, piece)], row_recv.at[origin, piece],
                neighbour(way) * 2 + core,
            )

        def level_slot(goal, same, below):
            if not same:
                return goal
            return jnp.where(below, goal, nodes + lax.rem(goal, 2))

        def gathered(q, rel, piece):
            across = pieces[piece][0] == 0
            views = []
            goal = to_node(q, rel)
            waits = []
            if across and rel == 1:
                return views
            if (q == position and rel == 0) or (across and rel == 0):
                spot = to_level(q)
                waits.append((from_side, spot, side_recv))
            if q >= position and position > 0:
                slot = level_slot(goal, q == position, jnp.logical_not(flipped))
                waits.append((from_level, slot, level_recv))
            if q <= position:
                slot = level_slot(goal, q == position, flipped)
                waits.append((from_level, slot, level_recv))
            for ref, slot, recv in waits:
                view = ref.at[region(slot, piece)]
                remote(view, view, send_sem.at[0], recv.at[slot, piece], twin).wait_recv()
                row = region(slot, piece)[0]
                views.append(lambda at, ref=ref, row=row: ref[row, at])
            return views

        def collect(q, rel, piece):
            if (q, rel, piece) in dealt:
                return
            dealt.add((q, rel, piece))
            views = gathered(q, rel, piece)
            if not views:
                return
            spot = region(to_node(q, rel), piece)

            def store(at, value):
                partial[spot[0], at] = value.astype(jnp.bfloat16)

            strips(spot, partial, views, store)

        def pass_sum(q, rel, piece, way):
            collect(q, rel, piece)
            goal = to_node(q, rel)
            spot = region(goal, piece)
            if way == 2:
                slot = to_level(q)
                dst, recv = from_side.at[region(slot, piece)], side_recv.at[slot, piece]
            else:
                beside = position + (1 if way == 0 else -1)
                below = jnp.logical_not(flipped) if way == 0 else flipped
                slot = level_slot(goal, beside == q, below)
                dst, recv = from_level.at[region(slot, piece)], level_recv.at[slot, piece]
            push(partial.at[spot], dst, recv, neighbour(way) * 2 + core)

        def finish(q, rel, piece):
            views = gathered(q, rel, piece)
            spot = region(to_node(q, rel), piece)
            local = region(0, piece)[0]
            views = views + [lambda at: shared[local, at], lambda at: middle[local, at]]

            def store(at, value):
                out[local, at] = value.astype(jnp.bfloat16)

            strips(spot, partial, views, store)

        def slices(block):
            found = []
            for q, groups in block:
                for rel in (0, 1):
                    base = to_node(q, rel) * rows
                    runs = []
                    for g in groups:
                        if runs and runs[-1][1] == g:
                            runs[-1][1] = g + 1
                        else:
                            runs.append([g, g + 1])
                    for begin, end in runs:
                        size = (end - begin) * 2 * tile
                        at = pl.multiple_of(base + begin * 2 * tile, tile)
                        found.append((pl.ds(at, size), size))
            return found

        def block_in(block):
            for q, groups in block:
                for rel in (0, 1):
                    for piece, spec in enumerate(pieces):
                        if spec[1] // 2 in groups:
                            row_in(q, rel, piece)
            spots = slices(block)
            take = sum(size for _, size in spots)

            def source():
                return jnp.concatenate([rows_all[at, :] for at, _ in spots], axis=0)

            def gates(n):
                cols = pl.ds(pl.multiple_of(lax.rem(n, halves) * 256, 256), 256)
                return gate[n // halves, :, cols], up[n // halves, :, cols]

            def factor(n, value):
                lines = jnp.concatenate([scale[n // halves, at, :] for at, _ in spots], axis=0)
                return value * jnp.concatenate([lines, lines], axis=1)

            held[block] = min(set(range(depths)) - set(held.values()))
            feed_in(held[block] * 4 * rows, source, take, gates, 2 * halves, factor)

        def block_out(block):
            spots = slices(block)
            take = sum(size for _, size in spots)

            def keep(cols, piece):
                at = 0
                for spot, size in spots:
                    partial[spot, cols] = piece[at:at + size]
                    at += size

            feed_out(held.pop(block) * 4 * rows, take, 2 * hid, down, keep)

        begun = False
        ended = False
        for act in program:
            kind = act[0]
            if kind == 0:
                pass_row(*act[1:])
            elif kind == 1:
                pass_sum(*act[1:])
            elif kind == 2:
                finish(*act[1:])
            elif kind == 3:
                if not begun:
                    begun = True
                    spread_table()
                    for load in loads[3:5]:
                        load.wait()
                    twin_ready(0)
                    twin_ready(1)
                block_in(act[1])
            elif kind == 4:
                if not ended:
                    ended = True
                    loads[5].wait()
                    twin_ready(2)
                block_out(act[1])
            elif kind == 5:
                for copy in twins:
                    copy.start()
                rows_all[pl.ds(pl.multiple_of(node * rows, tile), rows), :] = own[...]
                shared_expert()
        for copy in sends:
            copy.wait_send()


    for position, program in enumerate(programs):
        near_end = jnp.logical_or(level == position, level == top - position)
        pl.when(near_end)(functools.partial(run, program, position))
    for copy in always + twins:
        copy.wait_send()


def plane_stage(
    second_normed, middle, routes, route_weights,
    expert_gate, expert_up, expert_down, shared_gate, shared_up, shared_down,
):
    experts = lax.axis_size("ep")
    nodes = experts // 2
    rows, width = second_normed.shape
    hid = expert_gate.shape[2]
    tiles = 6
    chosen = routes[None, :, :] == jnp.arange(experts, dtype=jnp.int32)[:, None, None]
    weights = jnp.sum(jnp.where(chosen, route_weights[None], 0.0), axis=2)
    weights = jnp.pad(weights, ((0, 0), (0, 128 - rows)))[:, None, :]
    vmem = pl.BlockSpec(memory_space=pltpu.VMEM)
    hbm = pl.BlockSpec(memory_space=pl.ANY)
    dma = pltpu.SemaphoreType.DMA
    half = jnp.bfloat16
    programs, pieces = PLAN
    count = len(pieces)
    most = max(sum(act[0] < 2 for act in program) for program in programs)
    return pl.pallas_call(
        functools.partial(plane_kernel, PLAN, tiles),
        out_shape=jax.ShapeDtypeStruct((rows, width), half),
        in_specs=[vmem] * 3 + [hbm] * 6,
        out_specs=vmem,
        scratch_shapes=[
            pltpu.VMEM((nodes * rows, width), half),
            pltpu.VMEM((nodes * rows, width), half),
            pltpu.VMEM(((nodes + 2) * rows, width), half),
            pltpu.VMEM((nodes // 2 * rows, width), half),
            pltpu.VMEM((nodes, 2, 1, 128), jnp.float32),
            pltpu.VMEM((2, nodes * rows, 128), jnp.float32),
            pltpu.VMEM((2, width, hid), half),
            pltpu.VMEM((2, width, hid), half),
            pltpu.VMEM((2 * hid, width), half),
            pltpu.VMEM(shared_gate.shape, half),
            pltpu.VMEM(shared_up.shape, half),
            pltpu.VMEM(shared_down.shape, half),
            pltpu.VMEM((3 * 4 * rows, 2 * hid), half),
            pltpu.VMEM((rows, width), half),
            dma((6,)),
            dma((3,)),
            dma((3,)),
            dma((nodes,)),
            dma((nodes,)),
            dma((nodes, count)),
            dma((nodes + 2, count)),
            dma((nodes // 2, count)),
            dma((most,)),
        ],
        compiler_params=pltpu.CompilerParams(
            collective_id=0, has_side_effects=True, vmem_limit_bytes=60 * 1024 * 1024
        ),
    )(
        second_normed, middle, weights,
        expert_gate, expert_up, expert_down, shared_gate, shared_up, shared_down,
    )


def mixer_kernel(
    tokens, prior, mix_gain, in_weight, params, input_map, output_map, skip, out_weight,
    channel_gain, new_state, middle, second, normed, acts, acc,
):
    step = pl.program_id(0)
    lane = 128
    channels = in_weight.shape[1]
    width = input_map.shape[2]
    group = acts.shape[1] * width // prior.shape[2]
    per = lane // group
    states = per * width

    def scaled(values, gain):
        factor = lax.rsqrt(jnp.mean(values * values, axis=-1, keepdims=True) + norm_eps)
        return (values * factor * gain[...]).astype(jnp.bfloat16)

    @pl.when(step == 0)
    def _():
        normed[...] = scaled(tokens[...].astype(jnp.float32), mix_gain)
        acc[...] = jnp.zeros_like(acc)

    drive = jnp.dot(normed[...], in_weight[...], preferred_element_type=jnp.float32)
    drive = drive.astype(jnp.bfloat16)
    row = lax.broadcasted_iota(jnp.int32, (lane, states), 0) // group
    column = lax.broadcasted_iota(jnp.int32, (lane, states), 1) // width
    own_group = row == column

    def spread(table):
        tiled = jnp.concatenate([table] * per, axis=1)
        return jnp.where(own_group, tiled, 0.0).astype(jnp.bfloat16)

    for sub in range(channels // lane):
        cols = slice(sub * lane, (sub + 1) * lane)
        ent = slice(sub * states, (sub + 1) * states)
        part = drive[:, cols]
        push_real = jnp.dot(
            part, spread(input_map[0, cols, :]), preferred_element_type=jnp.float32
        )
        push_imag = jnp.dot(
            part, spread(input_map[1, cols, :]), preferred_element_type=jnp.float32
        )
        turn_real, turn_imag = params[0:1, ent], params[1:2, ent]
        hold_real, hold_imag = params[2:3, ent], params[3:4, ent]
        old_real, old_imag = prior[0, :, ent], prior[1, :, ent]
        fresh_real = (
            turn_real * old_real - turn_imag * old_imag
            + (push_real * hold_real - push_imag * hold_imag)
        )
        fresh_imag = (
            turn_real * old_imag + turn_imag * old_real
            + (push_real * hold_imag + push_imag * hold_real)
        )
        new_state[0, :, ent] = fresh_real
        new_state[1, :, ent] = fresh_imag
        across = (((1,), (1,)), ((), ()))
        readout = lax.dot_general(
            fresh_real.astype(jnp.bfloat16), spread(output_map[0, cols, :]), across,
            preferred_element_type=jnp.float32,
        ) - lax.dot_general(
            fresh_imag.astype(jnp.bfloat16), spread(output_map[1, cols, :]), across,
            preferred_element_type=jnp.float32,
        )
        readout = readout + skip[:, cols] * part.astype(jnp.float32)
        acts[:, cols] = jax.nn.gelu(readout).astype(jnp.bfloat16)
    acc[...] += jnp.dot(acts[...], out_weight[...], preferred_element_type=jnp.float32)

    @pl.when(step == pl.num_programs(0) - 1)
    def _():
        mixed = acc[...].astype(jnp.bfloat16).astype(jnp.float32)
        mid = (tokens[...].astype(jnp.float32) + mixed).astype(jnp.bfloat16)
        middle[...] = mid
        second[...] = scaled(mid.astype(jnp.float32), channel_gain)


def mixer_stage(
    tokens, prior_state, mix_gain, in_weight, decay_rate, frequency, log_step,
    input_map, output_map, skip_gain, out_weight, channel_gain,
):
    rows, model = tokens.shape
    groups, width = decay_rate.shape
    channels = in_weight.shape[1]
    step_size = jnp.exp(log_step)[:, None]
    real_rate = -decay_rate
    magnitude = jnp.exp(real_rate * step_size)
    turn_real = magnitude * jnp.cos(frequency * step_size)
    turn_imag = magnitude * jnp.sin(frequency * step_size)
    denominator = real_rate * real_rate + frequency * frequency
    hold_real = ((turn_real - 1.0) * real_rate + turn_imag * frequency) / denominator
    hold_imag = (turn_imag * real_rate - (turn_real - 1.0) * frequency) / denominator
    params = jnp.stack([turn_real, turn_imag, hold_real, hold_imag]).reshape(4, -1)
    in_map = jnp.transpose(input_map, (0, 1, 3, 2)).reshape(2, channels, width)
    out_map = output_map.reshape(2, channels, width)
    block = 256
    states = block * groups * width // channels

    def whole(*shape):
        return pl.BlockSpec(shape, lambda i: (0,) * len(shape))

    half = jnp.bfloat16
    return pl.pallas_call(
        mixer_kernel,
        grid=(channels // block,),
        out_shape=(
            jax.ShapeDtypeStruct(prior_state.shape, jnp.float32),
            jax.ShapeDtypeStruct((rows, model), half),
            jax.ShapeDtypeStruct((rows, model), half),
        ),
        in_specs=[
            whole(rows, model),
            pl.BlockSpec((2, rows, states), lambda i: (0, 0, i)),
            whole(1, model),
            pl.BlockSpec((model, block), lambda i: (0, i)),
            pl.BlockSpec((4, states), lambda i: (0, i)),
            pl.BlockSpec((2, block, width), lambda i: (0, i, 0)),
            pl.BlockSpec((2, block, width), lambda i: (0, i, 0)),
            pl.BlockSpec((1, block), lambda i: (0, i)),
            pl.BlockSpec((block, model), lambda i: (i, 0)),
            whole(1, model),
        ],
        out_specs=(
            pl.BlockSpec((2, rows, states), lambda i: (0, 0, i)),
            whole(rows, model),
            whole(rows, model),
        ),
        scratch_shapes=[
            pltpu.VMEM((rows, model), half),
            pltpu.VMEM((rows, block), half),
            pltpu.VMEM((rows, model), jnp.float32),
        ],
        compiler_params=pltpu.CompilerParams(
            dimension_semantics=("arbitrary",), vmem_limit_bytes=62 * 1024 * 1024
        ),
    )(
        tokens, prior_state, mix_gain[None], in_weight, params, in_map, out_map,
        skip_gain[None], out_weight, channel_gain[None],
    )


def body(
    tokens,
    prior_state,
    mix_gain,
    in_weight,
    decay_rate,
    frequency,
    log_step,
    input_map,
    output_map,
    skip_gain,
    out_weight,
    channel_gain,
    expert_gate,
    expert_up,
    expert_down,
    shared_gate,
    shared_up,
    shared_down,
    routes,
    route_weights,
):
    if lax.axis_size("tp") == 1 and lax.axis_size("ep") == 16:
        new_state, middle, second_normed = mixer_stage(
            tokens, prior_state, mix_gain, in_weight, decay_rate, frequency, log_step,
            input_map, output_map, skip_gain, out_weight, channel_gain,
        )
        layer_out = plane_stage(
            second_normed, middle, routes, route_weights,
            expert_gate, expert_up, expert_down, shared_gate, shared_up, shared_down,
        )
        return (layer_out, new_state)
    normed = root_scale(tokens, mix_gain)
    drive_rows = jnp.dot(normed, in_weight, preferred_element_type=jnp.float32).astype(jnp.bfloat16)
    readout, new_state = state_update(
        drive_rows, prior_state, decay_rate, frequency, log_step, input_map, output_map, skip_gain
    )
    activated = jax.nn.gelu(readout).astype(jnp.bfloat16)
    partial_value = jnp.dot(activated, out_weight, preferred_element_type=jnp.float32)
    mixer_out = lax.psum(partial_value.astype(jnp.bfloat16), "tp").astype(jnp.float32)
    middle = (tokens.astype(jnp.float32) + mixer_out).astype(jnp.bfloat16)
    second_normed = root_scale(middle, channel_gain)
    shared_gval = jnp.dot(second_normed, shared_gate, preferred_element_type=jnp.float32)
    shared_uval = jnp.dot(second_normed, shared_up, preferred_element_type=jnp.float32)
    shared_hidden = (jax.nn.silu(shared_gval) * shared_uval).astype(jnp.bfloat16)
    shared_piece = jnp.dot(shared_hidden, shared_down, preferred_element_type=jnp.float32)
    shared_out = lax.psum_scatter(
        shared_piece.astype(jnp.bfloat16), "tp", scatter_dimension=1, tiled=True
    ).astype(jnp.float32)
    half_cols = second_normed.shape[1] // lax.axis_size("tp")
    routed = exchanged_experts(
        second_normed, routes, route_weights, expert_gate, expert_up, expert_down
    )
    own_middle = lax.dynamic_slice_in_dim(middle, lax.axis_index("tp") * half_cols, half_cols, 1)
    layer_out = (own_middle.astype(jnp.float32) + routed + shared_out).astype(jnp.bfloat16)
    return (layer_out, new_state)


def solution(mesh):
    in_specs = (
        P(("grp", "ep"), None),
        P(None, ("grp", "ep"), "tp"),
        P(),
        P(None, "tp"),
        P("tp", None),
        P("tp", None),
        P("tp"),
        P(None, "tp", None, None),
        P(None, "tp", None, None),
        P("tp"),
        P("tp", None),
        P(),
        P("ep", None, "tp"),
        P("ep", None, "tp"),
        P("ep", "tp", None),
        P(None, "tp"),
        P(None, "tp"),
        P("tp", None),
        P(("grp", "ep"), None),
        P(("grp", "ep"), None),
    )
    out_specs = (P(("grp", "ep"), "tp"), P(None, ("grp", "ep"), "tp"))
    return jax.shard_map(body, mesh=mesh, in_specs=in_specs, out_specs=out_specs, check_vma=False)
```

```python
import functools
import jax
import jax.numpy as jnp
from jax import lax
from jax.experimental import pallas as pl
from jax.experimental.pallas import tpu as pltpu
from jax.sharding import PartitionSpec as P

norm_eps = 1e-06
highest = lax.Precision.HIGHEST
MESH = pl.DeviceIdType.MESH


def root_scale(activations, scale_gain):
    values = activations.astype(jnp.float32)
    factor = lax.rsqrt(jnp.mean(values * values, axis=-1, keepdims=True) + norm_eps)
    return (values * factor * scale_gain).astype(jnp.bfloat16)


def state_update(
    drive_rows, prior_state, decay_rate, frequency, log_step, input_map, output_map, skip_gain
):
    sequences = drive_rows.shape[0]
    groups = decay_rate.shape[0]
    driven = drive_rows.astype(jnp.float32).reshape(sequences, groups, -1)
    step_size = jnp.exp(log_step)[:, None]
    real_rate = -decay_rate
    magnitude = jnp.exp(real_rate * step_size)
    turn_real = magnitude * jnp.cos(frequency * step_size)
    turn_imag = magnitude * jnp.sin(frequency * step_size)
    denominator = real_rate * real_rate + frequency * frequency
    hold_real = ((turn_real - 1.0) * real_rate + turn_imag * frequency) / denominator
    hold_imag = (turn_imag * real_rate - (turn_real - 1.0) * frequency) / denominator
    push_real = jnp.einsum("sgh,gph->sgp", driven, input_map[0], precision=highest)
    push_imag = jnp.einsum("sgh,gph->sgp", driven, input_map[1], precision=highest)
    enter_real = push_real * hold_real - push_imag * hold_imag
    enter_imag = push_real * hold_imag + push_imag * hold_real
    old_real = prior_state[0].reshape(sequences, groups, -1)
    old_imag = prior_state[1].reshape(sequences, groups, -1)
    fresh_real = turn_real * old_real - turn_imag * old_imag + enter_real
    fresh_imag = turn_real * old_imag + turn_imag * old_real + enter_imag
    readout = jnp.einsum("ghp,sgp->sgh", output_map[0], fresh_real, precision=highest)
    readout = readout - jnp.einsum("ghp,sgp->sgh", output_map[1], fresh_imag, precision=highest)
    readout = readout.reshape(sequences, -1) + skip_gain * drive_rows.astype(jnp.float32)
    fresh = jnp.stack([fresh_real.reshape(sequences, -1), fresh_imag.reshape(sequences, -1)])
    return (readout, fresh)


def exchanged_experts(second_normed, routes, route_weights, expert_gate, expert_up, expert_down):
    experts = lax.axis_size("ep")
    seq_rows, top_count = routes.shape
    slot_cap = min(seq_rows, max(2, 3 * seq_rows * top_count // (2 * experts)))
    flat_routes = routes.reshape(-1)
    one_hot = (flat_routes[:, None] == jnp.arange(experts, dtype=jnp.int32)[None, :]).astype(
        jnp.int32
    )
    ranked = jnp.sum((jnp.cumsum(one_hot, axis=0) - one_hot) * one_hot, axis=1)
    slot_index = flat_routes * slot_cap + ranked
    placed = slot_index[:, None] == jnp.arange(experts * slot_cap, dtype=jnp.int32)[None, :]
    placed_rows = jnp.any(placed.reshape(seq_rows, top_count, experts * slot_cap), axis=1).astype(
        jnp.bfloat16
    )
    outgoing = lax.dot_general(
        placed_rows, second_normed, (((0,), (0,)), ((), ())), preferred_element_type=jnp.float32
    ).astype(jnp.bfloat16)
    outgoing = outgoing.reshape(experts, slot_cap, -1)
    arrived = lax.all_to_all(outgoing, "ep", split_axis=0, concat_axis=0, tiled=True)
    sources, count_items, full_width = arrived.shape
    expert_rows = arrived.reshape(sources * count_items, full_width)
    gate_val = jnp.dot(expert_rows, expert_gate[0], preferred_element_type=jnp.float32)
    up_val = jnp.dot(expert_rows, expert_up[0], preferred_element_type=jnp.float32)
    hidden = (jax.nn.silu(gate_val) * up_val).astype(jnp.bfloat16)
    piece = jnp.dot(hidden, expert_down[0], preferred_element_type=jnp.float32)
    summed = lax.psum_scatter(
        piece.reshape(sources, count_items, full_width).astype(jnp.bfloat16),
        "tp",
        scatter_dimension=2,
        tiled=True,
    )
    returned = lax.all_to_all(summed, "ep", split_axis=0, concat_axis=0, tiled=True)
    flat_back = returned.reshape(experts * slot_cap, -1)
    picked = (
        jnp.take(flat_back, slot_index, axis=0).reshape(seq_rows, top_count, -1).astype(jnp.float32)
    )
    routed = jnp.einsum("sk,skd->sd", route_weights, picked)
    return routed


PIECES = (
    (1, 0, 1, 0, 8),
    (0, 1, 1, 0, 8),
    (1, 2, 1, 0, 8),
    (0, 3, 1, 0, 8),
    (0, 4, 1, 0, 8),
    (0, 5, 1, 0, 4),
    (1, 5, 1, 4, 4),
)

END_PROGRAM = (
    (0, 0, 0, 0, 2), (0, 0, 0, 0, 0), (0, 0, 0, 1, 2), (0, 0, 0, 1, 0), (0, 0, 0, 3, 2),
    (0, 0, 0, 2, 2), (0, 0, 0, 3, 0), (5,), (0, 0, 1, 0, 0), (0, 0, 0, 2, 0), (0, 0, 0, 4, 0),
    (0, 1, 0, 1, 2), (0, 1, 0, 3, 2), (0, 0, 0, 4, 2), (0, 0, 1, 2, 0), (0, 0, 0, 5, 0),
    (0, 0, 0, 6, 0), (0, 2, 0, 1, 2), (0, 0, 0, 5, 2), (0, 0, 0, 6, 2),
    (3, ((0, (1,)), (1, (0,)))), (4, ((0, (1,)), (1, (0,)))), (1, 1, 0, 0, 0), (1, 1, 1, 0, 0),
    (1, 1, 1, 1, 2), (0, 3, 0, 1, 2), (1, 0, 1, 3, 2), (0, 0, 1, 6, 0), (3, ((2, (0,)),)),
    (4, ((2, (0,)),)), (1, 2, 0, 0, 0), (1, 2, 1, 0, 0), (1, 2, 1, 1, 2), (1, 1, 0, 1, 0),
    (0, 3, 0, 3, 2), (3, ((3, (0,)),)), (0, 2, 0, 3, 2), (4, ((3, (0,)),)), (1, 3, 0, 0, 0),
    (1, 3, 1, 0, 0), (1, 3, 1, 1, 2), (1, 2, 0, 1, 0), (3, ((0, (0,)), (3, (1,)))),
    (4, ((0, (0,)), (3, (1,)))), (1, 3, 0, 2, 0), (1, 3, 1, 2, 0), (1, 3, 1, 3, 2),
    (1, 0, 1, 1, 2), (3, ((2, (1,)),)), (1, 3, 0, 1, 0), (4, ((2, (1,)),)), (1, 2, 0, 2, 0),
    (1, 2, 1, 2, 0), (1, 2, 1, 3, 2), (0, 3, 0, 4, 2), (0, 3, 0, 5, 2), (1, 3, 0, 3, 0),
    (3, ((1, (1,)),)), (0, 2, 0, 4, 2), (4, ((1, (1,)),)), (1, 2, 0, 3, 0), (1, 1, 0, 2, 0),
    (1, 1, 1, 3, 2), (0, 2, 0, 5, 2), (3, ((3, (2,)),)), (0, 1, 0, 4, 2), (4, ((3, (2,)),)),
    (1, 3, 0, 6, 0), (1, 3, 1, 4, 2), (1, 3, 1, 5, 2), (0, 1, 0, 5, 2), (1, 3, 1, 6, 0),
    (1, 1, 1, 2, 0), (3, ((2, (2,)),)), (4, ((2, (2,)),)), (1, 2, 0, 6, 0), (1, 2, 1, 4, 2),
    (1, 2, 1, 5, 2), (1, 2, 1, 6, 0), (1, 3, 0, 4, 0), (1, 0, 1, 2, 2), (1, 3, 0, 5, 0),
    (1, 1, 0, 3, 0), (3, ((0, (2,)), (1, (2,)))), (4, ((0, (2,)), (1, (2,)))), (1, 2, 0, 4, 0),
    (1, 1, 0, 6, 0), (1, 1, 1, 4, 2), (1, 1, 1, 6, 0), (1, 0, 1, 0, 2), (1, 1, 1, 5, 2),
    (1, 0, 1, 4, 2), (1, 2, 0, 5, 0), (2, 0, 0, 2), (2, 0, 0, 1), (2, 0, 0, 0), (1, 0, 1, 6, 2),
    (1, 0, 1, 5, 2), (1, 1, 0, 4, 0), (1, 1, 0, 5, 0), (2, 0, 0, 3), (2, 0, 0, 6), (2, 0, 0, 4),
    (2, 0, 0, 5),
)

MID_PROGRAM = (
    (0, 1, 0, 0, 2), (0, 1, 0, 0, 0), (0, 1, 0, 0, 1), (0, 1, 0, 1, 2), (0, 1, 0, 1, 0),
    (0, 1, 0, 1, 1), (0, 1, 0, 3, 2), (0, 1, 0, 2, 2), (0, 1, 0, 3, 0), (0, 1, 0, 3, 1), (5,),
    (0, 0, 0, 0, 0), (0, 2, 0, 0, 1), (0, 0, 0, 1, 2), (0, 0, 0, 1, 0), (0, 1, 1, 0, 0),
    (0, 2, 0, 1, 2), (0, 2, 0, 1, 1), (0, 1, 1, 0, 1), (0, 0, 0, 3, 2), (0, 0, 1, 0, 0),
    (0, 0, 0, 3, 0), (0, 3, 0, 0, 1), (0, 0, 0, 2, 0), (0, 3, 0, 1, 2), (0, 2, 0, 3, 2),
    (0, 3, 0, 1, 1), (0, 0, 0, 4, 2), (0, 2, 1, 0, 1), (0, 0, 1, 2, 0), (0, 1, 0, 2, 0),
    (0, 1, 1, 2, 0), (0, 0, 0, 4, 0), (0, 3, 1, 0, 1), (0, 0, 0, 5, 0), (0, 1, 0, 4, 0),
    (0, 1, 0, 5, 0), (0, 3, 0, 3, 2), (0, 0, 0, 5, 2), (0, 1, 0, 4, 2), (0, 1, 0, 5, 2),
    (0, 1, 0, 6, 2), (0, 3, 0, 3, 1), (0, 2, 0, 3, 1), (0, 0, 0, 6, 0), (0, 3, 0, 2, 1),
    (0, 3, 1, 2, 1), (0, 2, 0, 2, 1), (0, 0, 1, 6, 0), (0, 1, 0, 6, 0),
    (3, ((0, (2,)), (3, (1,)))), (0, 2, 1, 2, 1), (4, ((0, (2,)), (3, (1,)))), (0, 3, 0, 4, 2),
    (0, 3, 0, 4, 1), (1, 3, 1, 3, 2), (1, 0, 1, 4, 2), (1, 0, 1, 5, 2), (0, 1, 1, 6, 0),
    (0, 3, 0, 5, 1), (0, 1, 0, 2, 1), (0, 1, 1, 2, 1), (3, ((1, (1, 2)), (2, (0,)), (3, (0,)))),
    (0, 2, 0, 4, 1), (0, 2, 0, 5, 1), (4, ((1, (1, 2)), (2, (0,)), (3, (0,)))), (0, 3, 0, 6, 1),
    (0, 3, 1, 6, 1), (0, 1, 0, 4, 1), (0, 1, 0, 5, 1), (1, 3, 1, 1, 2), (1, 2, 0, 0, 0),
    (1, 2, 1, 1, 2), (0, 3, 0, 5, 2), (1, 1, 1, 3, 2), (0, 2, 0, 4, 2), (0, 2, 0, 5, 2),
    (1, 1, 1, 4, 2), (1, 1, 1, 5, 2), (1, 3, 0, 0, 0), (0, 2, 0, 6, 1), (0, 2, 1, 6, 1),
    (0, 1, 0, 6, 1), (0, 1, 1, 6, 1), (1, 3, 1, 0, 0), (1, 2, 1, 0, 0), (1, 3, 0, 2, 0),
    (1, 3, 1, 2, 0), (1, 2, 0, 1, 0), (3, ((0, (1,)), (1, (0,)), (2, (1,)), (3, (2,)))),
    (1, 3, 0, 1, 0), (4, ((0, (1,)), (1, (0,)), (2, (1,)), (3, (2,)))), (1, 3, 1, 4, 2),
    (1, 3, 1, 5, 2), (1, 0, 0, 2, 1), (1, 2, 0, 2, 0), (1, 2, 1, 2, 0), (1, 1, 1, 0, 2),
    (3, ((0, (0,)), (2, (2,)))), (1, 3, 0, 3, 0), (1, 0, 1, 2, 1), (4, ((0, (0,)), (2, (2,)))),
    (1, 0, 0, 0, 1), (1, 0, 1, 0, 1), (1, 0, 1, 1, 2), (1, 0, 1, 3, 2), (1, 2, 1, 3, 2),
    (1, 3, 0, 6, 0), (1, 3, 1, 6, 0), (2, 1, 0, 0), (1, 1, 1, 2, 2), (1, 2, 1, 4, 2),
    (1, 2, 1, 5, 2), (1, 1, 1, 1, 2), (1, 0, 0, 1, 1), (1, 2, 0, 6, 0), (1, 2, 1, 6, 0),
    (1, 0, 0, 6, 1), (1, 0, 1, 6, 1), (1, 0, 0, 3, 1), (1, 3, 0, 4, 0), (1, 3, 0, 5, 0),
    (1, 2, 0, 3, 0), (2, 1, 0, 2), (1, 2, 0, 4, 0), (1, 0, 0, 4, 1), (1, 0, 0, 5, 1),
    (1, 1, 1, 6, 2), (2, 1, 0, 1), (1, 2, 0, 5, 0), (2, 1, 0, 3), (2, 1, 0, 6), (2, 1, 0, 4),
    (2, 1, 0, 5),
)

PLAN = ((END_PROGRAM, MID_PROGRAM), PIECES)


def plane_kernel(
    plan, tiles,
    own, middle, routes, route_weights, gate_in, up_in, down_in, sgate_in, sup_in, sdown_in,
    out,
    weights, rows_all, partial, from_level, from_side, table, scale,
    gate, up, down, sgate, sup, sdown, hidden, shared,
    load_sem, twin_send, twin_recv, w_send, w_recv,
    row_recv, level_recv, side_recv, send_sem,
):
    programs, pieces = plan
    experts = lax.axis_size("ep")
    me = lax.axis_index("ep")
    core = lax.rem(me, 2)
    node = me // 2
    col = lax.rem(node, 2)
    level = node // 2
    nodes = experts // 2
    top = nodes // 2 - 1
    rows, width = own.shape
    tile = rows // tiles
    hid = sgate.shape[1]
    flipped = level * 2 > top
    upward = jnp.where(flipped, -1, 1)
    twin = node * 2 + 1 - core

    def to_level(q):
        return jnp.where(flipped, top - q, q)

    def to_col(rel):
        return col if rel == 0 else 1 - col

    def to_node(q, rel):
        return to_level(q) * 2 + to_col(rel)

    def region(base, piece):
        at, high, left, wide = pieces[piece][1:]
        return (
            pl.ds(pl.multiple_of(base * rows + at * tile, tile), high * tile),
            pl.ds(left * width // 8, wide * width // 8),
        )

    loads = [
        pltpu.make_async_copy(src, dst, load_sem.at[n])
        for n, (src, dst) in enumerate(
            (
                (sgate_in, sgate), (sup_in, sup), (sdown_in, sdown),
                (gate_in.at[0], gate.at[core]), (up_in.at[0], up.at[core]),
                (down_in.at[0], down.at[pl.ds(pl.multiple_of(core * hid, hid), hid)]),
            )
        )
    ]
    for load in loads:
        load.start()

    barrier = pltpu.get_barrier_semaphore()
    for step in range(1, experts):
        pl.semaphore_signal(
            barrier, inc=1, device_id={"ep": lax.rem(me + step, experts)}, device_id_type=MESH
        )
    expert = lax.broadcasted_iota(jnp.int32, (experts, rows), 0)
    chosen = jnp.zeros((experts, rows), jnp.float32)
    for k in range(routes.shape[0]):
        chosen = chosen + jnp.where(expert == routes[k:k + 1, :], route_weights[k:k + 1, :], 0.0)
    weights[...] = jnp.zeros_like(weights)
    for n in range(nodes):
        weights[n, 0:2, 0:rows] = chosen[2 * n:2 * n + 2]
    pl.semaphore_wait(barrier, experts - 1)

    def remote(src, dst, send, recv, target):
        return pltpu.make_async_remote_copy(
            src_ref=src, dst_ref=dst, send_sem=send, recv_sem=recv,
            device_id={"ep": target}, device_id_type=MESH,
        )

    always = []
    for step in range(1, nodes):
        other = lax.rem(node + step, nodes)
        copy = remote(
            weights.at[other], table.at[node],
            w_send.at[step], w_recv.at[nodes - step], other * 2 + core,
        )
        copy.start()
        always.append(copy)
    twins = [
        remote(src, dst, twin_send.at[n], twin_recv.at[n], twin)
        for n, (src, dst) in enumerate(
            (
                (gate_in.at[0], gate.at[core]), (up_in.at[0], up.at[core]),
                (down_in.at[0], down.at[pl.ds(pl.multiple_of(core * hid, hid), hid)]),
            )
        )
    ]

    def twin_ready(n):
        refs = (gate.at[1 - core], up.at[1 - core],
                down.at[pl.ds(pl.multiple_of((1 - core) * hid, hid), hid)])
        remote(refs[n], refs[n], twin_send.at[n], twin_recv.at[n], twin).wait_recv()

    def strips(spot, first, others, store):
        row, lanes = spot
        wide = lanes.size
        step = 512 if wide % 512 == 0 else 256

        def strip(n, carry):
            at = pl.ds(pl.multiple_of(lanes.start + n * step, 128), step)
            value = first[row, at].astype(jnp.float32)
            for view in others:
                value = value + view(at).astype(jnp.float32)
            store(at, value)
            return carry

        lax.fori_loop(0, wide // step, strip, 0)

    def feed_in(base, source, take, gates, chunks, factor):
        def first(n, carry):
            data = source()
            gate_w, up_w = gates(n)
            g = jnp.dot(data, gate_w, preferred_element_type=jnp.float32)
            u = jnp.dot(data, up_w, preferred_element_type=jnp.float32)
            at = pl.ds(pl.multiple_of(n * 256, 256), 256)
            hidden[pl.ds(base, take), at] = factor(n, jax.nn.silu(g) * u).astype(jnp.bfloat16)
            return carry

        lax.fori_loop(0, chunks, first, 0, unroll=True)

    def feed_out(base, take, depth, down_w, finish):
        def second(n, carry):
            cols = pl.ds(pl.multiple_of(n * 512, 512), 512)
            piece = jnp.dot(
                hidden[pl.ds(base, take), pl.ds(0, depth)], down_w[:, cols],
                preferred_element_type=jnp.float32,
            )
            finish(cols, piece.astype(jnp.bfloat16))
            return carry

        lax.fori_loop(0, width // 512, second, 0, unroll=True)

    halves = hid // 256
    depths = hidden.shape[0] // (4 * rows)

    def shared_expert():
        for load in loads[:3]:
            load.wait()

        def gates(n):
            cols = pl.ds(pl.multiple_of(n * 256, 256), 256)
            return sgate[:, cols], sup[:, cols]

        feed_in(0, lambda: own[...], rows, gates, halves, lambda n, value: value)

        def keep(cols, piece):
            shared[:, cols] = piece

        feed_out(0, rows, hid, sdown, keep)

    def spread_table():
        for step in range(1, nodes):
            other = lax.rem(node + step, nodes)
            remote(
                table.at[other], table.at[other], w_send.at[step], w_recv.at[step], twin
            ).wait_recv()
        table[node] = weights[node]

        def one(n, carry):
            for e in range(2):
                line = jnp.broadcast_to(table[n, e:e + 1, :], (128, 128))
                scale[e, pl.ds(pl.multiple_of(n * rows, tile), rows), :] = jnp.transpose(line)[:rows]
            return carry

        lax.fori_loop(0, nodes, one, 0)

    def run(program, position):
        sends = []
        landed = set()
        dealt = set()
        held = {}

        def push(src, dst, recv, target):
            copy = remote(src, dst, send_sem.at[len(sends)], recv, target)
            copy.start()
            sends.append(copy)

        def row_in(q, rel, piece):
            if (q, rel) == (position, 0) or (q, rel, piece) in landed:
                return
            landed.add((q, rel, piece))
            origin = to_node(q, rel)
            view = rows_all.at[region(origin, piece)]
            remote(view, view, send_sem.at[0], row_recv.at[origin, piece], twin).wait_recv()

        def neighbour(way):
            if way == 2:
                return level * 2 + 1 - col
            return (level + (upward if way == 0 else -upward)) * 2 + col

        def pass_row(q, rel, piece, way):
            row_in(q, rel, piece)
            origin = to_node(q, rel)
            if (q, rel) == (position, 0):
                src = own.at[region(0, piece)]
            else:
                src = rows_all.at[region(origin, piece)]
            push(
                src, rows_all.at[region(origin, piece)], row_recv.at[origin, piece],
                neighbour(way) * 2 + core,
            )

        def level_slot(goal, same, below):
            if not same:
                return goal
            return jnp.where(below, goal, nodes + lax.rem(goal, 2))

        def gathered(q, rel, piece):
            across = pieces[piece][0] == 0
            views = []
            goal = to_node(q, rel)
            waits = []
            if across and rel == 1:
                return views
            if (q == position and rel == 0) or (across and rel == 0):
                spot = to_level(q)
                waits.append((from_side, spot, side_recv))
            if q >= position and position > 0:
                slot = level_slot(goal, q == position, jnp.logical_not(flipped))
                waits.append((from_level, slot, level_recv))
            if q <= position:
                slot = level_slot(goal, q == position, flipped)
                waits.append((from_level, slot, level_recv))
            for ref, slot, recv in waits:
                view = ref.at[region(slot, piece)]
                remote(view, view, send_sem.at[0], recv.at[slot, piece], twin).wait_recv()
                row = region(slot, piece)[0]
                views.append(lambda at, ref=ref, row=row: ref[row, at])
            return views

        def collect(q, rel, piece):
            if (q, rel, piece) in dealt:
                return
            dealt.add((q, rel, piece))
            views = gathered(q, rel, piece)
            if not views:
                return
            spot = region(to_node(q, rel), piece)

            def store(at, value):
                partial[spot[0], at] = value.astype(jnp.bfloat16)

            strips(spot, partial, views, store)

        def pass_sum(q, rel, piece, way):
            collect(q, rel, piece)
            goal = to_node(q, rel)
            spot = region(goal, piece)
            if way == 2:
                slot = to_level(q)
                dst, recv = from_side.at[region(slot, piece)], side_recv.at[slot, piece]
            else:
                beside = position + (1 if way == 0 else -1)
                below = jnp.logical_not(flipped) if way == 0 else flipped
                slot = level_slot(goal, beside == q, below)
                dst, recv = from_level.at[region(slot, piece)], level_recv.at[slot, piece]
            push(partial.at[spot], dst, recv, neighbour(way) * 2 + core)

        def finish(q, rel, piece):
            views = gathered(q, rel, piece)
            spot = region(to_node(q, rel), piece)
            local = region(0, piece)[0]
            views = views + [lambda at: shared[local, at], lambda at: middle[local, at]]

            def store(at, value):
                out[local, at] = value.astype(jnp.bfloat16)

            strips(spot, partial, views, store)

        def slices(block):
            found = []
            for q, groups in block:
                for rel in (0, 1):
                    base = to_node(q, rel) * rows
                    runs = []
                    for g in groups:
                        if runs and runs[-1][1] == g:
                            runs[-1][1] = g + 1
                        else:
                            runs.append([g, g + 1])
                    for begin, end in runs:
                        size = (end - begin) * 2 * tile
                        at = pl.multiple_of(base + begin * 2 * tile, tile)
                        found.append((pl.ds(at, size), size))
            return found

        def block_in(block):
            for q, groups in block:
                for rel in (0, 1):
                    for piece, spec in enumerate(pieces):
                        if spec[1] // 2 in groups:
                            row_in(q, rel, piece)
            spots = slices(block)
            take = sum(size for _, size in spots)

            def source():
                return jnp.concatenate([rows_all[at, :] for at, _ in spots], axis=0)

            def gates(n):
                cols = pl.ds(pl.multiple_of(lax.rem(n, halves) * 256, 256), 256)
                return gate[n // halves, :, cols], up[n // halves, :, cols]

            def factor(n, value):
                lines = jnp.concatenate([scale[n // halves, at, :] for at, _ in spots], axis=0)
                return value * jnp.concatenate([lines, lines], axis=1)

            held[block] = min(set(range(depths)) - set(held.values()))
            feed_in(held[block] * 4 * rows, source, take, gates, 2 * halves, factor)

        def block_out(block):
            spots = slices(block)
            take = sum(size for _, size in spots)

            def keep(cols, piece):
                at = 0
                for spot, size in spots:
                    partial[spot, cols] = piece[at:at + size]
                    at += size

            feed_out(held.pop(block) * 4 * rows, take, 2 * hid, down, keep)

        begun = False
        ended = False
        for act in program:
            kind = act[0]
            if kind == 0:
                pass_row(*act[1:])
            elif kind == 1:
                pass_sum(*act[1:])
            elif kind == 2:
                finish(*act[1:])
            elif kind == 3:
                if not begun:
                    begun = True
                    spread_table()
                    for load in loads[3:5]:
                        load.wait()
                    twin_ready(0)
                    twin_ready(1)
                block_in(act[1])
            elif kind == 4:
                if not ended:
                    ended = True
                    loads[5].wait()
                    twin_ready(2)
                block_out(act[1])
            elif kind == 5:
                for copy in twins:
                    copy.start()
                rows_all[pl.ds(pl.multiple_of(node * rows, tile), rows), :] = own[...]
                shared_expert()
        for copy in sends:
            copy.wait_send()


    for position, program in enumerate(programs):
        near_end = jnp.logical_or(level == position, level == top - position)
        pl.when(near_end)(functools.partial(run, program, position))
    for copy in always + twins:
        copy.wait_send()


def plane_stage(
    second_normed, middle, routes, route_weights,
    expert_gate, expert_up, expert_down, shared_gate, shared_up, shared_down,
):
    experts = lax.axis_size("ep")
    nodes = experts // 2
    rows, width = second_normed.shape
    hid = expert_gate.shape[2]
    tiles = 6
    vmem = pl.BlockSpec(memory_space=pltpu.VMEM)
    hbm = pl.BlockSpec(memory_space=pl.ANY)
    dma = pltpu.SemaphoreType.DMA
    half = jnp.bfloat16
    programs, pieces = PLAN
    count = len(pieces)
    most = max(sum(act[0] < 2 for act in program) for program in programs)
    return pl.pallas_call(
        functools.partial(plane_kernel, PLAN, tiles),
        out_shape=jax.ShapeDtypeStruct((rows, width), half),
        in_specs=[vmem] * 4 + [hbm] * 6,
        out_specs=vmem,
        scratch_shapes=[
            pltpu.VMEM((nodes, 8, 128), jnp.float32),
            pltpu.VMEM((nodes * rows, width), half),
            pltpu.VMEM((nodes * rows, width), half),
            pltpu.VMEM(((nodes + 2) * rows, width), half),
            pltpu.VMEM((nodes // 2 * rows, width), half),
            pltpu.VMEM((nodes, 8, 128), jnp.float32),
            pltpu.VMEM((2, nodes * rows, 128), jnp.float32),
            pltpu.VMEM((2, width, hid), half),
            pltpu.VMEM((2, width, hid), half),
            pltpu.VMEM((2 * hid, width), half),
            pltpu.VMEM(shared_gate.shape, half),
            pltpu.VMEM(shared_up.shape, half),
            pltpu.VMEM(shared_down.shape, half),
            pltpu.VMEM((3 * 4 * rows, 2 * hid), half),
            pltpu.VMEM((rows, width), half),
            dma((6,)),
            dma((3,)),
            dma((3,)),
            dma((nodes,)),
            dma((nodes,)),
            dma((nodes, count)),
            dma((nodes + 2, count)),
            dma((nodes // 2, count)),
            dma((most,)),
        ],
        compiler_params=pltpu.CompilerParams(
            collective_id=0, has_side_effects=True, vmem_limit_bytes=65011712
        ),
    )(
        second_normed, middle, routes.T, route_weights.T,
        expert_gate, expert_up, expert_down, shared_gate, shared_up, shared_down,
    )


def mixer_kernel(
    tokens_in, prior_in, mix_gain_in, in_weight_in, decay_in, frequency_in, log_step_in,
    input_map_in, output_map_in, skip_in, out_weight_in, channel_gain_in,
    new_state, middle, second,
    tokens, prior, mix_gain, in_weight, decay, frequency, log_step,
    input_map, output_map, skip, out_weight, channel_gain,
    params, table, normed, acts, first_sem, chunk_sem, tail_sem, out_sem,
):
    lane = 128
    chunks, model, block = in_weight.shape
    rows = tokens.shape[0]
    groups, width = decay.shape
    states = prior.shape[3]
    group = chunks * block // groups
    per = lane // group
    entries = per * width

    firsts = [
        pltpu.make_async_copy(src, dst, first_sem.at[n])
        for n, (src, dst) in enumerate(
            ((tokens_in, tokens), (mix_gain_in, mix_gain), (decay_in, decay),
             (frequency_in, frequency), (log_step_in, log_step), (skip_in, skip),
             (channel_gain_in, channel_gain))
        )
    ]

    def chunk_copies(k):
        cols = pl.ds(pl.multiple_of(k * block, block), block)
        wide = pl.ds(pl.multiple_of(k * states, states), states)
        return [
            pltpu.make_async_copy(src, dst, chunk_sem.at[n, k])
            for n, (src, dst) in enumerate(
                ((in_weight_in.at[:, cols], in_weight.at[k]),
                 (input_map_in.at[:, cols], input_map.at[k]),
                 (output_map_in.at[:, cols], output_map.at[k]),
                 (prior_in.at[:, :, wide], prior.at[k]))
            )
        ]

    def leaving(k):
        wide = pl.ds(pl.multiple_of(k * states, states), states)
        return pltpu.make_async_copy(prior.at[k], new_state.at[:, :, wide], out_sem.at[k])

    for copy in firsts:
        copy.start()
    for k in range(chunks):
        for copy in chunk_copies(k):
            copy.start()
    tail = pltpu.make_async_copy(out_weight_in, out_weight, tail_sem.at[0])
    tail.start()

    def scaled(values, gain):
        factor = lax.rsqrt(jnp.mean(values * values, axis=-1, keepdims=True) + norm_eps)
        return (values * factor * gain[...]).astype(jnp.bfloat16)

    for copy in firsts[2:]:
        copy.wait()
    diagonal = lax.broadcasted_iota(jnp.int32, (groups, groups), 0) == (
        lax.broadcasted_iota(jnp.int32, (groups, groups), 1)
    )
    steps = jnp.where(diagonal, jnp.broadcast_to(log_step[...], (groups, groups)), 0.0)
    step_size = jnp.exp(jnp.sum(steps, axis=1, keepdims=True))
    real_rate = -decay[...]
    angle = frequency[...] * step_size
    magnitude = jnp.exp(real_rate * step_size)
    turn_real = magnitude * jnp.cos(angle)
    turn_imag = magnitude * jnp.sin(angle)
    denominator = real_rate * real_rate + frequency[...] * frequency[...]
    params[0] = turn_real
    params[1] = turn_imag
    params[2] = ((turn_real - 1.0) * real_rate + turn_imag * frequency[...]) / denominator
    params[3] = (turn_imag * real_rate - (turn_real - 1.0) * frequency[...]) / denominator
    for copy in firsts[:2]:
        copy.wait()
    normed[...] = scaled(tokens[...].astype(jnp.float32), mix_gain)
    for n in range(4):
        for g in range(0, groups, 2):
            pair = jnp.concatenate([params[n, g:g + 1, :], params[n, g + 1:g + 2, :]], axis=1)
            table[n:n + 1, g * width:(g + 2) * width] = pair

    row = lax.broadcasted_iota(jnp.int32, (lane, entries), 0) // group
    column = lax.broadcasted_iota(jnp.int32, (lane, entries), 1) // width
    own_group = row == column

    def spread(values):
        tiled = jnp.concatenate([values] * per, axis=1)
        return jnp.where(own_group, tiled, 0.0).astype(jnp.bfloat16)

    across = (((1,), (1,)), ((), ()))

    def chunk(k, carry):
        for copy in chunk_copies(k):
            copy.wait()
        drive = jnp.dot(normed[...], in_weight[k], preferred_element_type=jnp.float32)
        drive = drive.astype(jnp.bfloat16)
        for sub in range(block // lane):
            cols = slice(sub * lane, (sub + 1) * lane)
            ent = slice(sub * entries, (sub + 1) * entries)
            at = pl.ds(pl.multiple_of(k * states + sub * entries, entries), entries)
            spot = pl.ds(pl.multiple_of(k * block + sub * lane, lane), lane)
            part = drive[:, cols]
            push_real = jnp.dot(
                part, spread(input_map[k, 0, cols, :]), preferred_element_type=jnp.float32
            )
            push_imag = jnp.dot(
                part, spread(input_map[k, 1, cols, :]), preferred_element_type=jnp.float32
            )
            turn_real, turn_imag = table[0:1, at], table[1:2, at]
            hold_real, hold_imag = table[2:3, at], table[3:4, at]
            old_real, old_imag = prior[k, 0, :, ent], prior[k, 1, :, ent]
            fresh_real = (
                turn_real * old_real - turn_imag * old_imag
                + (push_real * hold_real - push_imag * hold_imag)
            )
            fresh_imag = (
                turn_real * old_imag + turn_imag * old_real
                + (push_real * hold_imag + push_imag * hold_real)
            )
            prior[k, 0, :, ent] = fresh_real
            prior[k, 1, :, ent] = fresh_imag
            readout = lax.dot_general(
                fresh_real.astype(jnp.bfloat16), spread(output_map[k, 0, cols, :]), across,
                preferred_element_type=jnp.float32,
            ) - lax.dot_general(
                fresh_imag.astype(jnp.bfloat16), spread(output_map[k, 1, cols, :]), across,
                preferred_element_type=jnp.float32,
            )
            readout = readout + skip[:, spot] * part.astype(jnp.float32)
            acts[:, spot] = jax.nn.gelu(readout).astype(jnp.bfloat16)
        leaving(k).start()
        return carry

    lax.fori_loop(0, chunks, chunk, 0)
    tail.wait()
    wide = 512
    total = jnp.zeros((rows, 1), jnp.float32)
    for n in range(model // wide):
        cols = slice(n * wide, (n + 1) * wide)
        mixed = jnp.dot(acts[...], out_weight[:, cols], preferred_element_type=jnp.float32)
        mixed = mixed.astype(jnp.bfloat16).astype(jnp.float32)
        mid = (tokens[:, cols].astype(jnp.float32) + mixed).astype(jnp.bfloat16)
        middle[:, cols] = mid
        mid = mid.astype(jnp.float32)
        total = total + jnp.sum(mid * mid, axis=-1, keepdims=True)
    factor = lax.rsqrt(total / model + norm_eps)
    for n in range(model // wide):
        cols = slice(n * wide, (n + 1) * wide)
        mid = middle[:, cols].astype(jnp.float32)
        second[:, cols] = (mid * factor * channel_gain[:, cols]).astype(jnp.bfloat16)
    for k in range(chunks):
        leaving(k).wait()


def mixer_stage(
    tokens, prior_state, mix_gain, in_weight, decay_rate, frequency, log_step,
    input_map, output_map, skip_gain, out_weight, channel_gain,
):
    rows, model = tokens.shape
    groups, width = decay_rate.shape
    channels = in_weight.shape[1]
    in_map = jnp.transpose(input_map, (0, 1, 3, 2)).reshape(2, channels, width)
    out_map = output_map.reshape(2, channels, width)
    block = 256
    chunks = channels // block
    states = block * groups * width // channels
    half = jnp.bfloat16
    full = jnp.float32
    hbm = pl.BlockSpec(memory_space=pl.ANY)
    vmem = pl.BlockSpec(memory_space=pltpu.VMEM)
    dma = pltpu.SemaphoreType.DMA
    return pl.pallas_call(
        mixer_kernel,
        out_shape=(
            jax.ShapeDtypeStruct(prior_state.shape, full),
            jax.ShapeDtypeStruct((rows, model), half),
            jax.ShapeDtypeStruct((rows, model), half),
        ),
        in_specs=[hbm] * 12,
        out_specs=(hbm, vmem, vmem),
        scratch_shapes=[
            pltpu.VMEM((rows, model), half),
            pltpu.VMEM((chunks, 2, rows, states), full),
            pltpu.VMEM((1, model), full),
            pltpu.VMEM((chunks, model, block), half),
            pltpu.VMEM((groups, width), full),
            pltpu.VMEM((groups, width), full),
            pltpu.VMEM((1, groups), full),
            pltpu.VMEM((chunks, 2, block, width), full),
            pltpu.VMEM((chunks, 2, block, width), full),
            pltpu.VMEM((1, channels), full),
            pltpu.VMEM((channels, model), half),
            pltpu.VMEM((1, model), full),
            pltpu.VMEM((4, groups, width), full),
            pltpu.VMEM((4, groups * width), full),
            pltpu.VMEM((rows, model), half),
            pltpu.VMEM((rows, channels), half),
            dma((7,)),
            dma((4, chunks)),
            dma((1,)),
            dma((chunks,)),
        ],
        compiler_params=pltpu.CompilerParams(vmem_limit_bytes=65011712),
    )(
        tokens, prior_state, mix_gain[None], in_weight, decay_rate, frequency, log_step[None],
        in_map, out_map, skip_gain[None], out_weight, channel_gain[None],
    )


def body(
    tokens,
    prior_state,
    mix_gain,
    in_weight,
    decay_rate,
    frequency,
    log_step,
    input_map,
    output_map,
    skip_gain,
    out_weight,
    channel_gain,
    expert_gate,
    expert_up,
    expert_down,
    shared_gate,
    shared_up,
    shared_down,
    routes,
    route_weights,
):
    if lax.axis_size("tp") == 1 and lax.axis_size("ep") == 16:
        new_state, middle, second_normed = mixer_stage(
            tokens, prior_state, mix_gain, in_weight, decay_rate, frequency, log_step,
            input_map, output_map, skip_gain, out_weight, channel_gain,
        )
        layer_out = plane_stage(
            second_normed, middle, routes, route_weights,
            expert_gate, expert_up, expert_down, shared_gate, shared_up, shared_down,
        )
        return (layer_out, new_state)
    normed = root_scale(tokens, mix_gain)
    drive_rows = jnp.dot(normed, in_weight, preferred_element_type=jnp.float32).astype(jnp.bfloat16)
    readout, new_state = state_update(
        drive_rows, prior_state, decay_rate, frequency, log_step, input_map, output_map, skip_gain
    )
    activated = jax.nn.gelu(readout).astype(jnp.bfloat16)
    partial_value = jnp.dot(activated, out_weight, preferred_element_type=jnp.float32)
    mixer_out = lax.psum(partial_value.astype(jnp.bfloat16), "tp").astype(jnp.float32)
    middle = (tokens.astype(jnp.float32) + mixer_out).astype(jnp.bfloat16)
    second_normed = root_scale(middle, channel_gain)
    shared_gval = jnp.dot(second_normed, shared_gate, preferred_element_type=jnp.float32)
    shared_uval = jnp.dot(second_normed, shared_up, preferred_element_type=jnp.float32)
    shared_hidden = (jax.nn.silu(shared_gval) * shared_uval).astype(jnp.bfloat16)
    shared_piece = jnp.dot(shared_hidden, shared_down, preferred_element_type=jnp.float32)
    shared_out = lax.psum_scatter(
        shared_piece.astype(jnp.bfloat16), "tp", scatter_dimension=1, tiled=True
    ).astype(jnp.float32)
    half_cols = second_normed.shape[1] // lax.axis_size("tp")
    routed = exchanged_experts(
        second_normed, routes, route_weights, expert_gate, expert_up, expert_down
    )
    own_middle = lax.dynamic_slice_in_dim(middle, lax.axis_index("tp") * half_cols, half_cols, 1)
    layer_out = (own_middle.astype(jnp.float32) + routed + shared_out).astype(jnp.bfloat16)
    return (layer_out, new_state)


def solution(mesh):
    in_specs = (
        P(("grp", "ep"), None),
        P(None, ("grp", "ep"), "tp"),
        P(),
        P(None, "tp"),
        P("tp", None),
        P("tp", None),
        P("tp"),
        P(None, "tp", None, None),
        P(None, "tp", None, None),
        P("tp"),
        P("tp", None),
        P(),
        P("ep", None, "tp"),
        P("ep", None, "tp"),
        P("ep", "tp", None),
        P(None, "tp"),
        P(None, "tp"),
        P("tp", None),
        P(("grp", "ep"), None),
        P(("grp", "ep"), None),
    )
    out_specs = (P(("grp", "ep"), "tp"), P(None, ("grp", "ep"), "tp"))
    return jax.shard_map(body, mesh=mesh, in_specs=in_specs, out_specs=out_specs, check_vma=False)
```

```python
import functools
import jax
import jax.numpy as jnp
from jax import lax
from jax.experimental import pallas as pl
from jax.experimental.pallas import tpu as pltpu
from jax.sharding import PartitionSpec as P

norm_eps = 1e-06
highest = lax.Precision.HIGHEST
MESH = pl.DeviceIdType.MESH


def root_scale(activations, scale_gain):
    values = activations.astype(jnp.float32)
    factor = lax.rsqrt(jnp.mean(values * values, axis=-1, keepdims=True) + norm_eps)
    return (values * factor * scale_gain).astype(jnp.bfloat16)


def state_update(
    drive_rows, prior_state, decay_rate, frequency, log_step, input_map, output_map, skip_gain
):
    sequences = drive_rows.shape[0]
    groups = decay_rate.shape[0]
    driven = drive_rows.astype(jnp.float32).reshape(sequences, groups, -1)
    step_size = jnp.exp(log_step)[:, None]
    real_rate = -decay_rate
    magnitude = jnp.exp(real_rate * step_size)
    turn_real = magnitude * jnp.cos(frequency * step_size)
    turn_imag = magnitude * jnp.sin(frequency * step_size)
    denominator = real_rate * real_rate + frequency * frequency
    hold_real = ((turn_real - 1.0) * real_rate + turn_imag * frequency) / denominator
    hold_imag = (turn_imag * real_rate - (turn_real - 1.0) * frequency) / denominator
    push_real = jnp.einsum("sgh,gph->sgp", driven, input_map[0], precision=highest)
    push_imag = jnp.einsum("sgh,gph->sgp", driven, input_map[1], precision=highest)
    enter_real = push_real * hold_real - push_imag * hold_imag
    enter_imag = push_real * hold_imag + push_imag * hold_real
    old_real = prior_state[0].reshape(sequences, groups, -1)
    old_imag = prior_state[1].reshape(sequences, groups, -1)
    fresh_real = turn_real * old_real - turn_imag * old_imag + enter_real
    fresh_imag = turn_real * old_imag + turn_imag * old_real + enter_imag
    readout = jnp.einsum("ghp,sgp->sgh", output_map[0], fresh_real, precision=highest)
    readout = readout - jnp.einsum("ghp,sgp->sgh", output_map[1], fresh_imag, precision=highest)
    readout = readout.reshape(sequences, -1) + skip_gain * drive_rows.astype(jnp.float32)
    fresh = jnp.stack([fresh_real.reshape(sequences, -1), fresh_imag.reshape(sequences, -1)])
    return (readout, fresh)


def exchanged_experts(second_normed, routes, route_weights, expert_gate, expert_up, expert_down):
    experts = lax.axis_size("ep")
    seq_rows, top_count = routes.shape
    slot_cap = min(seq_rows, max(2, 3 * seq_rows * top_count // (2 * experts)))
    flat_routes = routes.reshape(-1)
    one_hot = (flat_routes[:, None] == jnp.arange(experts, dtype=jnp.int32)[None, :]).astype(
        jnp.int32
    )
    ranked = jnp.sum((jnp.cumsum(one_hot, axis=0) - one_hot) * one_hot, axis=1)
    slot_index = flat_routes * slot_cap + ranked
    placed = slot_index[:, None] == jnp.arange(experts * slot_cap, dtype=jnp.int32)[None, :]
    placed_rows = jnp.any(placed.reshape(seq_rows, top_count, experts * slot_cap), axis=1).astype(
        jnp.bfloat16
    )
    outgoing = lax.dot_general(
        placed_rows, second_normed, (((0,), (0,)), ((), ())), preferred_element_type=jnp.float32
    ).astype(jnp.bfloat16)
    outgoing = outgoing.reshape(experts, slot_cap, -1)
    arrived = lax.all_to_all(outgoing, "ep", split_axis=0, concat_axis=0, tiled=True)
    sources, count_items, full_width = arrived.shape
    expert_rows = arrived.reshape(sources * count_items, full_width)
    gate_val = jnp.dot(expert_rows, expert_gate[0], preferred_element_type=jnp.float32)
    up_val = jnp.dot(expert_rows, expert_up[0], preferred_element_type=jnp.float32)
    hidden = (jax.nn.silu(gate_val) * up_val).astype(jnp.bfloat16)
    piece = jnp.dot(hidden, expert_down[0], preferred_element_type=jnp.float32)
    summed = lax.psum_scatter(
        piece.reshape(sources, count_items, full_width).astype(jnp.bfloat16),
        "tp",
        scatter_dimension=2,
        tiled=True,
    )
    returned = lax.all_to_all(summed, "ep", split_axis=0, concat_axis=0, tiled=True)
    flat_back = returned.reshape(experts * slot_cap, -1)
    picked = (
        jnp.take(flat_back, slot_index, axis=0).reshape(seq_rows, top_count, -1).astype(jnp.float32)
    )
    routed = jnp.einsum("sk,skd->sd", route_weights, picked)
    return routed


PIECES = (
    (1, 0, 1, 0, 8),
    (0, 1, 1, 0, 8),
    (1, 2, 1, 0, 8),
    (0, 3, 1, 0, 8),
    (0, 4, 1, 0, 8),
    (0, 5, 1, 0, 4),
    (1, 5, 1, 4, 4),
)

END_PROGRAM = (
    (0, 0, 0, 0, 2), (0, 0, 0, 0, 0), (0, 0, 0, 1, 2), (0, 0, 0, 1, 0), (0, 0, 0, 3, 2),
    (0, 0, 0, 2, 2), (0, 0, 0, 3, 0), (5,), (0, 0, 1, 0, 0), (0, 0, 0, 2, 0), (0, 0, 0, 4, 0),
    (0, 1, 0, 1, 2), (0, 1, 0, 3, 2), (0, 0, 0, 4, 2), (0, 0, 1, 2, 0), (0, 0, 0, 5, 0),
    (0, 0, 0, 6, 0), (0, 2, 0, 1, 2), (0, 0, 0, 5, 2), (0, 0, 0, 6, 2), (3, ((1, (0,)),)),
    (4, ((1, (0,)),)), (1, 1, 0, 0, 0), (1, 1, 1, 0, 0), (1, 1, 1, 1, 2), (0, 3, 0, 1, 2),
    (0, 0, 1, 6, 0), (3, ((2, (0,)),)), (4, ((2, (0,)),)), (1, 2, 0, 0, 0), (1, 2, 1, 0, 0),
    (1, 2, 1, 1, 2), (1, 1, 0, 1, 0), (0, 3, 0, 3, 2), (3, ((0, (1,)), (3, (0,)))),
    (0, 2, 0, 3, 2), (4, ((0, (1,)), (3, (0,)))), (1, 3, 0, 0, 0), (1, 3, 1, 0, 0),
    (1, 3, 1, 1, 2), (1, 0, 1, 3, 2), (1, 2, 0, 1, 0), (3, ((3, (1,)),)), (4, ((3, (1,)),)),
    (1, 3, 0, 2, 0), (1, 3, 1, 2, 0), (1, 3, 1, 3, 2), (3, ((0, (2,)), (2, (1,)))),
    (0, 3, 0, 4, 2), (1, 3, 0, 1, 0), (4, ((0, (2,)), (2, (1,)))), (1, 2, 1, 3, 2),
    (0, 3, 0, 5, 2), (1, 0, 1, 4, 2), (1, 3, 0, 3, 0), (1, 2, 0, 2, 0), (1, 2, 1, 2, 0),
    (3, ((1, (1,)),)), (0, 2, 0, 4, 2), (4, ((1, (1,)),)), (1, 2, 0, 3, 0), (1, 1, 1, 3, 2),
    (0, 2, 0, 5, 2), (1, 0, 1, 5, 2), (3, ((3, (2,)),)), (4, ((3, (2,)),)), (1, 3, 0, 6, 0),
    (1, 3, 1, 4, 2), (1, 3, 1, 5, 2), (0, 1, 0, 4, 2), (0, 1, 0, 5, 2), (1, 3, 1, 6, 0),
    (1, 1, 0, 2, 0), (1, 1, 1, 2, 0), (3, ((0, (0,)), (2, (2,)))), (4, ((0, (0,)), (2, (2,)))),
    (1, 2, 1, 4, 2), (1, 2, 1, 5, 2), (1, 3, 0, 4, 0), (1, 3, 0, 5, 0), (1, 2, 0, 6, 0),
    (1, 2, 1, 6, 0), (1, 1, 0, 3, 0), (1, 0, 1, 2, 2), (1, 0, 1, 1, 2), (3, ((1, (2,)),)),
    (1, 2, 0, 4, 0), (2, 0, 0, 3), (4, ((1, (2,)),)), (1, 2, 0, 5, 0), (1, 1, 0, 6, 0),
    (1, 1, 1, 4, 2), (1, 1, 1, 5, 2), (1, 1, 1, 6, 0), (2, 0, 0, 2), (1, 0, 1, 0, 2),
    (1, 0, 1, 6, 2), (1, 1, 0, 4, 0), (1, 1, 0, 5, 0), (2, 0, 0, 1), (2, 0, 0, 0), (2, 0, 0, 6),
    (2, 0, 0, 4), (2, 0, 0, 5),
)

MID_PROGRAM = (
    (0, 1, 0, 0, 2), (0, 1, 0, 0, 0), (0, 1, 0, 0, 1), (0, 1, 0, 1, 2), (0, 1, 0, 1, 0),
    (0, 1, 0, 1, 1), (0, 1, 0, 3, 2), (0, 1, 0, 2, 2), (0, 1, 0, 3, 0), (0, 1, 0, 3, 1), (5,),
    (0, 0, 0, 0, 0), (0, 2, 0, 0, 1), (0, 0, 0, 1, 2), (0, 0, 0, 1, 0), (0, 1, 1, 0, 0),
    (0, 2, 0, 1, 2), (0, 2, 0, 1, 1), (0, 1, 1, 0, 1), (0, 0, 0, 3, 2), (0, 0, 1, 0, 0),
    (0, 0, 0, 3, 0), (0, 3, 0, 0, 1), (0, 0, 0, 2, 0), (0, 3, 0, 1, 2), (0, 2, 0, 3, 2),
    (0, 3, 0, 1, 1), (0, 0, 0, 4, 2), (0, 2, 1, 0, 1), (0, 0, 1, 2, 0), (0, 1, 0, 2, 0),
    (0, 1, 1, 2, 0), (0, 0, 0, 4, 0), (0, 3, 1, 0, 1), (0, 0, 0, 5, 0), (0, 1, 0, 4, 0),
    (0, 1, 0, 5, 0), (0, 3, 0, 3, 2), (0, 0, 0, 5, 2), (0, 1, 0, 4, 2), (0, 1, 0, 5, 2),
    (0, 1, 0, 6, 2), (0, 3, 0, 3, 1), (0, 2, 0, 3, 1), (0, 0, 0, 6, 0), (0, 3, 0, 2, 1),
    (0, 3, 1, 2, 1), (0, 2, 0, 2, 1), (3, ((2, (0,)), (3, (0, 1)))), (0, 2, 1, 2, 1),
    (0, 0, 1, 6, 0), (0, 1, 0, 6, 0), (4, ((2, (0,)), (3, (0, 1)))), (0, 3, 0, 4, 2),
    (0, 3, 0, 4, 1), (1, 3, 1, 1, 2), (1, 3, 1, 3, 2), (1, 2, 1, 1, 2),
    (3, ((0, (1, 2)), (1, (1,)), (2, (1,)))), (0, 1, 1, 6, 0), (0, 3, 0, 5, 1), (0, 1, 0, 2, 1),
    (0, 1, 1, 2, 1), (0, 2, 0, 4, 1), (0, 2, 0, 5, 1), (1, 2, 0, 0, 0), (1, 2, 1, 0, 0),
    (4, ((0, (1, 2)), (1, (1,)), (2, (1,)))), (0, 3, 0, 6, 1), (0, 3, 1, 6, 1), (0, 1, 0, 4, 1),
    (0, 1, 0, 5, 1), (1, 2, 1, 3, 2), (1, 0, 1, 3, 2), (1, 0, 1, 4, 2), (1, 0, 1, 5, 2),
    (1, 1, 1, 3, 2), (0, 3, 0, 5, 2), (0, 2, 0, 4, 2), (0, 2, 0, 5, 2), (1, 3, 0, 0, 0),
    (0, 2, 0, 6, 1), (0, 2, 1, 6, 1), (0, 1, 0, 6, 1), (1, 3, 1, 0, 0), (1, 2, 0, 1, 0),
    (1, 3, 0, 2, 0), (1, 3, 1, 2, 0), (1, 3, 0, 1, 0), (1, 3, 0, 3, 0), (1, 0, 0, 2, 1),
    (0, 1, 1, 6, 1), (1, 2, 0, 2, 0), (3, ((1, (0, 2)), (3, (2,)))), (1, 0, 1, 2, 1),
    (1, 2, 1, 2, 0), (4, ((1, (0, 2)), (3, (2,)))), (1, 3, 1, 4, 2), (1, 3, 1, 5, 2),
    (1, 3, 0, 6, 0), (1, 2, 0, 3, 0), (1, 1, 1, 0, 2), (1, 0, 0, 3, 1),
    (3, ((0, (0,)), (2, (2,)))), (1, 3, 1, 6, 0), (4, ((0, (0,)), (2, (2,)))), (1, 0, 0, 0, 1),
    (1, 0, 1, 0, 1), (1, 0, 1, 1, 2), (1, 2, 1, 4, 2), (1, 2, 1, 5, 2), (1, 1, 1, 2, 2),
    (1, 1, 1, 1, 2), (1, 1, 1, 4, 2), (1, 1, 1, 5, 2), (1, 0, 0, 6, 1), (1, 3, 0, 4, 0),
    (1, 3, 0, 5, 0), (1, 0, 1, 6, 1), (2, 1, 0, 0), (1, 2, 0, 6, 0), (1, 2, 1, 6, 0),
    (1, 0, 0, 1, 1), (2, 1, 0, 3), (1, 0, 0, 4, 1), (1, 0, 0, 5, 1), (1, 2, 0, 4, 0),
    (1, 2, 0, 5, 0), (2, 1, 0, 2), (1, 1, 1, 6, 2), (2, 1, 0, 1), (2, 1, 0, 4), (2, 1, 0, 5),
    (2, 1, 0, 6),
)

PLAN = ((END_PROGRAM, MID_PROGRAM), PIECES)


def plane_kernel(
    plan, tiles,
    own_in, middle_in, routes_in, route_weights_in, gate_in, up_in, down_in, sgate_in, sup_in, sdown_in,
    out,
    middle, routes, route_weights, weights, rows_all, partial, from_level, from_side, table, scale,
    gate, up, down, sgate, sup, sdown, hidden, shared,
    load_sem, twin_send, twin_recv, w_send, w_recv,
    row_recv, level_recv, side_recv, send_sem, entry_sem,
):
    programs, pieces = plan
    experts = lax.axis_size("ep")
    me = lax.axis_index("ep")
    core = lax.rem(me, 2)
    node = me // 2
    col = lax.rem(node, 2)
    level = node // 2
    nodes = experts // 2
    top = nodes // 2 - 1
    rows, width = own_in.shape
    tile = rows // tiles
    hid = sgate.shape[1]
    flipped = level * 2 > top
    upward = jnp.where(flipped, -1, 1)
    twin = node * 2 + 1 - core

    def to_level(q):
        return jnp.where(flipped, top - q, q)

    def to_col(rel):
        return col if rel == 0 else 1 - col

    def to_node(q, rel):
        return to_level(q) * 2 + to_col(rel)

    def region(base, piece):
        at, high, left, wide = pieces[piece][1:]
        return (
            pl.ds(pl.multiple_of(base * rows + at * tile, tile), high * tile),
            pl.ds(left * width // 8, wide * width // 8),
        )

    loads = [
        pltpu.make_async_copy(src, dst, load_sem.at[n])
        for n, (src, dst) in enumerate(
            (
                (sgate_in, sgate), (sup_in, sup), (sdown_in, sdown),
                (gate_in.at[0], gate.at[core]), (up_in.at[0], up.at[core]),
                (down_in.at[0], down.at[pl.ds(pl.multiple_of(core * hid, hid), hid)]),
            )
        )
    ]
    home = pl.ds(pl.multiple_of(node * rows, tile), rows)
    entry = [
        pltpu.make_async_copy(src, dst, entry_sem.at[n])
        for n, (src, dst) in enumerate(
            ((own_in, rows_all.at[home]), (routes_in, routes),
             (route_weights_in, route_weights), (middle_in, middle))
        )
    ]
    for copy in entry + loads:
        copy.start()

    barrier = pltpu.get_barrier_semaphore()
    for step in range(1, experts):
        pl.semaphore_signal(
            barrier, inc=1, device_id={"ep": lax.rem(me + step, experts)}, device_id_type=MESH
        )
    entry[0].wait()
    pl.semaphore_wait(barrier, experts - 1)

    def remote(src, dst, send, recv, target):
        return pltpu.make_async_remote_copy(
            src_ref=src, dst_ref=dst, send_sem=send, recv_sem=recv,
            device_id={"ep": target}, device_id_type=MESH,
        )

    table_sends = [
        remote(
            weights.at[lax.rem(node + step, nodes)], table.at[node],
            w_send.at[step], w_recv.at[nodes - step],
            lax.rem(node + step, nodes) * 2 + core,
        )
        for step in range(1, nodes)
    ]

    def send_table():
        for copy in entry[1:]:
            copy.wait()
        expert = lax.broadcasted_iota(jnp.int32, (experts, rows), 0)
        chosen = jnp.zeros((experts, rows), jnp.float32)
        for k in range(routes.shape[0]):
            chosen = chosen + jnp.where(expert == routes[k:k + 1, :], route_weights[k:k + 1, :], 0.0)
        weights[...] = jnp.zeros_like(weights)
        for n in range(nodes):
            weights[n, 0:2, 0:rows] = chosen[2 * n:2 * n + 2]
        for copy in table_sends:
            copy.start()

    twins = [
        remote(src, dst, twin_send.at[n], twin_recv.at[n], twin)
        for n, (src, dst) in enumerate(
            (
                (gate_in.at[0], gate.at[core]), (up_in.at[0], up.at[core]),
                (down_in.at[0], down.at[pl.ds(pl.multiple_of(core * hid, hid), hid)]),
            )
        )
    ]

    def twin_ready(n):
        refs = (gate.at[1 - core], up.at[1 - core],
                down.at[pl.ds(pl.multiple_of((1 - core) * hid, hid), hid)])
        remote(refs[n], refs[n], twin_send.at[n], twin_recv.at[n], twin).wait_recv()

    def strips(spot, first, others, store):
        row, lanes = spot
        wide = lanes.size
        step = 512 if wide % 512 == 0 else 256

        def strip(n, carry):
            at = pl.ds(pl.multiple_of(lanes.start + n * step, 128), step)
            value = first[row, at].astype(jnp.float32)
            for view in others:
                value = value + view(at).astype(jnp.float32)
            store(at, value)
            return carry

        lax.fori_loop(0, wide // step, strip, 0)

    def feed_in(base, source, take, gates, chunks, factor):
        def first(n, carry):
            data = source()
            gate_w, up_w = gates(n)
            g = jnp.dot(data, gate_w, preferred_element_type=jnp.float32)
            u = jnp.dot(data, up_w, preferred_element_type=jnp.float32)
            at = pl.ds(pl.multiple_of(n * 256, 256), 256)
            hidden[pl.ds(base, take), at] = factor(n, jax.nn.silu(g) * u).astype(jnp.bfloat16)
            return carry

        lax.fori_loop(0, chunks, first, 0, unroll=True)

    def feed_out(base, take, depth, down_w, finish):
        def second(n, carry):
            cols = pl.ds(pl.multiple_of(n * 512, 512), 512)
            piece = jnp.dot(
                hidden[pl.ds(base, take), pl.ds(0, depth)], down_w[:, cols],
                preferred_element_type=jnp.float32,
            )
            finish(cols, piece.astype(jnp.bfloat16))
            return carry

        lax.fori_loop(0, width // 512, second, 0, unroll=True)

    halves = hid // 256
    depths = hidden.shape[0] // (4 * rows)

    def shared_expert():
        for load in loads[:3]:
            load.wait()

        def gates(n):
            cols = pl.ds(pl.multiple_of(n * 256, 256), 256)
            return sgate[:, cols], sup[:, cols]

        feed_in(0, lambda: rows_all[home, :], rows, gates, halves, lambda n, value: value)

        def keep(cols, piece):
            shared[:, cols] = piece

        feed_out(0, rows, hid, sdown, keep)

    def spread_table():
        for step in range(1, nodes):
            other = lax.rem(node + step, nodes)
            remote(
                table.at[other], table.at[other], w_send.at[step], w_recv.at[step], twin
            ).wait_recv()
        table[node] = weights[node]

        def one(n, carry):
            for e in range(2):
                line = jnp.broadcast_to(table[n, e:e + 1, :], (128, 128))
                scale[e, pl.ds(pl.multiple_of(n * rows, tile), rows), :] = jnp.transpose(line)[:rows]
            return carry

        lax.fori_loop(0, nodes, one, 0)

    def run(program, position):
        sends = []
        landed = set()
        dealt = set()
        held = {}

        def push(src, dst, recv, target):
            copy = remote(src, dst, send_sem.at[len(sends)], recv, target)
            copy.start()
            sends.append(copy)

        def row_in(q, rel, piece):
            if (q, rel) == (position, 0) or (q, rel, piece) in landed:
                return
            landed.add((q, rel, piece))
            origin = to_node(q, rel)
            view = rows_all.at[region(origin, piece)]
            remote(view, view, send_sem.at[0], row_recv.at[origin, piece], twin).wait_recv()

        def neighbour(way):
            if way == 2:
                return level * 2 + 1 - col
            return (level + (upward if way == 0 else -upward)) * 2 + col

        def pass_row(q, rel, piece, way):
            row_in(q, rel, piece)
            origin = to_node(q, rel)
            push(
                rows_all.at[region(origin, piece)], rows_all.at[region(origin, piece)],
                row_recv.at[origin, piece],
                neighbour(way) * 2 + core,
            )

        def level_slot(goal, same, below):
            if not same:
                return goal
            return jnp.where(below, goal, nodes + lax.rem(goal, 2))

        def gathered(q, rel, piece):
            across = pieces[piece][0] == 0
            views = []
            goal = to_node(q, rel)
            waits = []
            if across and rel == 1:
                return views
            if (q == position and rel == 0) or (across and rel == 0):
                spot = to_level(q)
                waits.append((from_side, spot, side_recv))
            if q >= position and position > 0:
                slot = level_slot(goal, q == position, jnp.logical_not(flipped))
                waits.append((from_level, slot, level_recv))
            if q <= position:
                slot = level_slot(goal, q == position, flipped)
                waits.append((from_level, slot, level_recv))
            for ref, slot, recv in waits:
                view = ref.at[region(slot, piece)]
                remote(view, view, send_sem.at[0], recv.at[slot, piece], twin).wait_recv()
                row = region(slot, piece)[0]
                views.append(lambda at, ref=ref, row=row: ref[row, at])
            return views

        def collect(q, rel, piece):
            if (q, rel, piece) in dealt:
                return
            dealt.add((q, rel, piece))
            views = gathered(q, rel, piece)
            if not views:
                return
            spot = region(to_node(q, rel), piece)

            def store(at, value):
                partial[spot[0], at] = value.astype(jnp.bfloat16)

            strips(spot, partial, views, store)

        def pass_sum(q, rel, piece, way):
            collect(q, rel, piece)
            goal = to_node(q, rel)
            spot = region(goal, piece)
            if way == 2:
                slot = to_level(q)
                dst, recv = from_side.at[region(slot, piece)], side_recv.at[slot, piece]
            else:
                beside = position + (1 if way == 0 else -1)
                below = jnp.logical_not(flipped) if way == 0 else flipped
                slot = level_slot(goal, beside == q, below)
                dst, recv = from_level.at[region(slot, piece)], level_recv.at[slot, piece]
            push(partial.at[spot], dst, recv, neighbour(way) * 2 + core)

        def finish(q, rel, piece):
            views = gathered(q, rel, piece)
            spot = region(to_node(q, rel), piece)
            local = region(0, piece)[0]
            views = views + [lambda at: shared[local, at], lambda at: middle[local, at]]

            def store(at, value):
                out[local, at] = value.astype(jnp.bfloat16)

            strips(spot, partial, views, store)

        def slices(block):
            found = []
            for q, groups in block:
                for rel in (0, 1):
                    base = to_node(q, rel) * rows
                    runs = []
                    for g in groups:
                        if runs and runs[-1][1] == g:
                            runs[-1][1] = g + 1
                        else:
                            runs.append([g, g + 1])
                    for begin, end in runs:
                        size = (end - begin) * 2 * tile
                        at = pl.multiple_of(base + begin * 2 * tile, tile)
                        found.append((pl.ds(at, size), size))
            return found

        def block_in(block):
            for q, groups in block:
                for rel in (0, 1):
                    for piece, spec in enumerate(pieces):
                        if spec[1] // 2 in groups:
                            row_in(q, rel, piece)
            spots = slices(block)
            take = sum(size for _, size in spots)

            def source():
                return jnp.concatenate([rows_all[at, :] for at, _ in spots], axis=0)

            def gates(n):
                cols = pl.ds(pl.multiple_of(lax.rem(n, halves) * 256, 256), 256)
                return gate[n // halves, :, cols], up[n // halves, :, cols]

            def factor(n, value):
                lines = jnp.concatenate([scale[n // halves, at, :] for at, _ in spots], axis=0)
                return value * jnp.concatenate([lines, lines], axis=1)

            held[block] = min(set(range(depths)) - set(held.values()))
            feed_in(held[block] * 4 * rows, source, take, gates, 2 * halves, factor)

        def block_out(block):
            spots = slices(block)
            take = sum(size for _, size in spots)

            def keep(cols, piece):
                at = 0
                for spot, size in spots:
                    partial[spot, cols] = piece[at:at + size]
                    at += size

            feed_out(held.pop(block) * 4 * rows, take, 2 * hid, down, keep)

        begun = False
        ended = False
        for act in program:
            kind = act[0]
            if kind == 0:
                pass_row(*act[1:])
            elif kind == 1:
                pass_sum(*act[1:])
            elif kind == 2:
                finish(*act[1:])
            elif kind == 3:
                if not begun:
                    begun = True
                    spread_table()
                    for load in loads[3:5]:
                        load.wait()
                    twin_ready(0)
                    twin_ready(1)
                block_in(act[1])
            elif kind == 4:
                if not ended:
                    ended = True
                    loads[5].wait()
                    twin_ready(2)
                block_out(act[1])
            elif kind == 5:
                for copy in twins:
                    copy.start()
                send_table()
                shared_expert()
        for copy in sends:
            copy.wait_send()


    for position, program in enumerate(programs):
        near_end = jnp.logical_or(level == position, level == top - position)
        pl.when(near_end)(functools.partial(run, program, position))
    for copy in table_sends + twins:
        copy.wait_send()


def plane_stage(
    second_normed, middle, routes, route_weights,
    expert_gate, expert_up, expert_down, shared_gate, shared_up, shared_down,
):
    experts = lax.axis_size("ep")
    nodes = experts // 2
    rows, width = second_normed.shape
    hid = expert_gate.shape[2]
    tiles = 6
    vmem = pl.BlockSpec(memory_space=pltpu.VMEM)
    hbm = pl.BlockSpec(memory_space=pl.ANY)
    dma = pltpu.SemaphoreType.DMA
    half = jnp.bfloat16
    programs, pieces = PLAN
    count = len(pieces)
    most = max(sum(act[0] < 2 for act in program) for program in programs)
    return pl.pallas_call(
        functools.partial(plane_kernel, PLAN, tiles),
        out_shape=jax.ShapeDtypeStruct((rows, width), half),
        in_specs=[hbm] * 10,
        out_specs=vmem,
        scratch_shapes=[
            pltpu.VMEM((rows, width), half),
            pltpu.VMEM((routes.shape[1], rows), jnp.int32),
            pltpu.VMEM((routes.shape[1], rows), jnp.float32),
            pltpu.VMEM((nodes, 8, 128), jnp.float32),
            pltpu.VMEM((nodes * rows, width), half),
            pltpu.VMEM((nodes * rows, width), half),
            pltpu.VMEM(((nodes + 2) * rows, width), half),
            pltpu.VMEM((nodes // 2 * rows, width), half),
            pltpu.VMEM((nodes, 8, 128), jnp.float32),
            pltpu.VMEM((2, nodes * rows, 128), jnp.float32),
            pltpu.VMEM((2, width, hid), half),
            pltpu.VMEM((2, width, hid), half),
            pltpu.VMEM((2 * hid, width), half),
            pltpu.VMEM(shared_gate.shape, half),
            pltpu.VMEM(shared_up.shape, half),
            pltpu.VMEM(shared_down.shape, half),
            pltpu.VMEM((3 * 4 * rows, 2 * hid), half),
            pltpu.VMEM((rows, width), half),
            dma((6,)),
            dma((3,)),
            dma((3,)),
            dma((nodes,)),
            dma((nodes,)),
            dma((nodes, count)),
            dma((nodes + 2, count)),
            dma((nodes // 2, count)),
            dma((most,)),
            dma((4,)),
        ],
        compiler_params=pltpu.CompilerParams(
            collective_id=0, has_side_effects=True, vmem_limit_bytes=62 * 1024 * 1024
        ),
    )(
        second_normed, middle, routes.T, route_weights.T,
        expert_gate, expert_up, expert_down, shared_gate, shared_up, shared_down,
    )


def mixer_kernel(
    tokens_in, prior_in, mix_gain_in, in_weight_in, decay_in, frequency_in, log_step_in,
    input_map_in, output_map_in, skip_in, out_weight_in, channel_gain_in,
    new_state, middle, second,
    tokens, prior, mix_gain, in_weight, decay, frequency, log_step,
    input_map, output_map, skip, out_weight, channel_gain,
    params, table, normed, acts, first_sem, chunk_sem, tail_sem, out_sem,
):
    lane = 128
    chunks, model, block = in_weight.shape
    rows = tokens.shape[0]
    groups, width = decay.shape
    states = prior.shape[3]
    group = chunks * block // groups
    per = lane // group
    entries = per * width

    firsts = [
        pltpu.make_async_copy(src, dst, first_sem.at[n])
        for n, (src, dst) in enumerate(
            ((tokens_in, tokens), (mix_gain_in, mix_gain), (decay_in, decay),
             (frequency_in, frequency), (log_step_in, log_step), (skip_in, skip),
             (channel_gain_in, channel_gain))
        )
    ]

    def chunk_copies(k):
        cols = pl.ds(pl.multiple_of(k * block, block), block)
        wide = pl.ds(pl.multiple_of(k * states, states), states)
        views = [
            (input_map_in.at[:, cols], input_map.at[k]),
            (output_map_in.at[:, cols], output_map.at[k]),
        ]
        for n in range(4):
            part = pl.ds(n * model // 4, model // 4)
            views.append((in_weight_in.at[part, cols], in_weight.at[k, part]))
        for n in range(2):
            views.append((prior_in.at[n, :, wide], prior.at[k, n]))
        return [
            pltpu.make_async_copy(src, dst, chunk_sem.at[n, k])
            for n, (src, dst) in enumerate(views)
        ]

    def leaving(k):
        wide = pl.ds(pl.multiple_of(k * states, states), states)
        return pltpu.make_async_copy(prior.at[k], new_state.at[:, :, wide], out_sem.at[k])

    def begin(k):
        for copy in chunk_copies(k):
            copy.start()

    tails = []
    for n in range(8):
        part = pl.ds(n * chunks * block // 8, chunks * block // 8)
        tails.append(
            pltpu.make_async_copy(out_weight_in.at[part], out_weight.at[part], tail_sem.at[n])
        )

    def begin_tail():
        for copy in tails:
            copy.start()

    for copy in firsts:
        copy.start()
    begin(0)
    begin(1)

    def scaled(values, gain):
        factor = lax.rsqrt(jnp.mean(values * values, axis=-1, keepdims=True) + norm_eps)
        return (values * factor * gain[...]).astype(jnp.bfloat16)

    for copy in firsts[2:]:
        copy.wait()
    diagonal = lax.broadcasted_iota(jnp.int32, (groups, groups), 0) == (
        lax.broadcasted_iota(jnp.int32, (groups, groups), 1)
    )
    steps = jnp.where(diagonal, jnp.broadcast_to(log_step[...], (groups, groups)), 0.0)
    step_size = jnp.exp(jnp.sum(steps, axis=1, keepdims=True))
    real_rate = -decay[...]
    angle = frequency[...] * step_size
    magnitude = jnp.exp(real_rate * step_size)
    turn_real = magnitude * jnp.cos(angle)
    turn_imag = magnitude * jnp.sin(angle)
    denominator = real_rate * real_rate + frequency[...] * frequency[...]
    params[0] = turn_real
    params[1] = turn_imag
    params[2] = ((turn_real - 1.0) * real_rate + turn_imag * frequency[...]) / denominator
    params[3] = (turn_imag * real_rate - (turn_real - 1.0) * frequency[...]) / denominator
    for copy in firsts[:2]:
        copy.wait()
    begin(2)
    normed[...] = scaled(tokens[...].astype(jnp.float32), mix_gain)
    for n in range(4):
        for g in range(0, groups, 2):
            pair = jnp.concatenate([params[n, g:g + 1, :], params[n, g + 1:g + 2, :]], axis=1)
            table[n:n + 1, g * width:(g + 2) * width] = pair

    row = lax.broadcasted_iota(jnp.int32, (lane, entries), 0) // group
    column = lax.broadcasted_iota(jnp.int32, (lane, entries), 1) // width
    own_group = row == column

    def spread(values):
        tiled = jnp.concatenate([values] * per, axis=1)
        return jnp.where(own_group, tiled, 0.0).astype(jnp.bfloat16)

    across = (((1,), (1,)), ((), ()))

    def chunk(k, carry):
        for copy in chunk_copies(k):
            copy.wait()
        pl.when(k + 3 < chunks)(lambda: begin(k + 3))
        pl.when(k + 3 == chunks)(begin_tail)
        drive = jnp.dot(normed[...], in_weight[k], preferred_element_type=jnp.float32)
        drive = drive.astype(jnp.bfloat16)
        for sub in range(block // lane):
            cols = slice(sub * lane, (sub + 1) * lane)
            ent = slice(sub * entries, (sub + 1) * entries)
            at = pl.ds(pl.multiple_of(k * states + sub * entries, entries), entries)
            spot = pl.ds(pl.multiple_of(k * block + sub * lane, lane), lane)
            part = drive[:, cols]
            push_real = jnp.dot(
                part, spread(input_map[k, 0, cols, :]), preferred_element_type=jnp.float32
            )
            push_imag = jnp.dot(
                part, spread(input_map[k, 1, cols, :]), preferred_element_type=jnp.float32
            )
            turn_real, turn_imag = table[0:1, at], table[1:2, at]
            hold_real, hold_imag = table[2:3, at], table[3:4, at]
            old_real, old_imag = prior[k, 0, :, ent], prior[k, 1, :, ent]
            fresh_real = (
                turn_real * old_real - turn_imag * old_imag
                + (push_real * hold_real - push_imag * hold_imag)
            )
            fresh_imag = (
                turn_real * old_imag + turn_imag * old_real
                + (push_real * hold_imag + push_imag * hold_real)
            )
            prior[k, 0, :, ent] = fresh_real
            prior[k, 1, :, ent] = fresh_imag
            readout = lax.dot_general(
                fresh_real.astype(jnp.bfloat16), spread(output_map[k, 0, cols, :]), across,
                preferred_element_type=jnp.float32,
            ) - lax.dot_general(
                fresh_imag.astype(jnp.bfloat16), spread(output_map[k, 1, cols, :]), across,
                preferred_element_type=jnp.float32,
            )
            readout = readout + skip[:, spot] * part.astype(jnp.float32)
            acts[:, spot] = jax.nn.gelu(readout).astype(jnp.bfloat16)
        leaving(k).start()
        return carry

    lax.fori_loop(0, chunks, chunk, 0)
    for copy in tails:
        copy.wait()
    wide = 512
    total = jnp.zeros((rows, 1), jnp.float32)
    for n in range(model // wide):
        cols = slice(n * wide, (n + 1) * wide)
        mixed = jnp.dot(acts[...], out_weight[:, cols], preferred_element_type=jnp.float32)
        mixed = mixed.astype(jnp.bfloat16).astype(jnp.float32)
        mid = (tokens[:, cols].astype(jnp.float32) + mixed).astype(jnp.bfloat16)
        middle[:, cols] = mid
        mid = mid.astype(jnp.float32)
        total = total + jnp.sum(mid * mid, axis=-1, keepdims=True)
    factor = lax.rsqrt(total / model + norm_eps)
    for n in range(model // wide):
        cols = slice(n * wide, (n + 1) * wide)
        mid = middle[:, cols].astype(jnp.float32)
        second[:, cols] = (mid * factor * channel_gain[:, cols]).astype(jnp.bfloat16)
    for k in range(chunks):
        leaving(k).wait()


def mixer_stage(
    tokens, prior_state, mix_gain, in_weight, decay_rate, frequency, log_step,
    input_map, output_map, skip_gain, out_weight, channel_gain,
):
    rows, model = tokens.shape
    groups, width = decay_rate.shape
    channels = in_weight.shape[1]
    in_map = jnp.transpose(input_map, (0, 1, 3, 2)).reshape(2, channels, width)
    out_map = output_map.reshape(2, channels, width)
    block = 256
    chunks = channels // block
    states = block * groups * width // channels
    half = jnp.bfloat16
    full = jnp.float32
    hbm = pl.BlockSpec(memory_space=pl.ANY)
    vmem = pl.BlockSpec(memory_space=pltpu.VMEM)
    dma = pltpu.SemaphoreType.DMA
    return pl.pallas_call(
        mixer_kernel,
        out_shape=(
            jax.ShapeDtypeStruct(prior_state.shape, full),
            jax.ShapeDtypeStruct((rows, model), half),
            jax.ShapeDtypeStruct((rows, model), half),
        ),
        in_specs=[hbm] * 12,
        out_specs=(hbm, vmem, vmem),
        scratch_shapes=[
            pltpu.VMEM((rows, model), half),
            pltpu.VMEM((chunks, 2, rows, states), full),
            pltpu.VMEM((1, model), full),
            pltpu.VMEM((chunks, model, block), half),
            pltpu.VMEM((groups, width), full),
            pltpu.VMEM((groups, width), full),
            pltpu.VMEM((1, groups), full),
            pltpu.VMEM((chunks, 2, block, width), full),
            pltpu.VMEM((chunks, 2, block, width), full),
            pltpu.VMEM((1, channels), full),
            pltpu.VMEM((channels, model), half),
            pltpu.VMEM((1, model), full),
            pltpu.VMEM((4, groups, width), full),
            pltpu.VMEM((4, groups * width), full),
            pltpu.VMEM((rows, model), half),
            pltpu.VMEM((rows, channels), half),
            dma((7,)),
            dma((8, chunks)),
            dma((8,)),
            dma((chunks,)),
        ],
        compiler_params=pltpu.CompilerParams(vmem_limit_bytes=62 * 1024 * 1024),
    )(
        tokens, prior_state, mix_gain[None], in_weight, decay_rate, frequency, log_step[None],
        in_map, out_map, skip_gain[None], out_weight, channel_gain[None],
    )


def body(
    tokens,
    prior_state,
    mix_gain,
    in_weight,
    decay_rate,
    frequency,
    log_step,
    input_map,
    output_map,
    skip_gain,
    out_weight,
    channel_gain,
    expert_gate,
    expert_up,
    expert_down,
    shared_gate,
    shared_up,
    shared_down,
    routes,
    route_weights,
):
    if lax.axis_size("tp") == 1 and lax.axis_size("ep") == 16:
        new_state, middle, second_normed = mixer_stage(
            tokens, prior_state, mix_gain, in_weight, decay_rate, frequency, log_step,
            input_map, output_map, skip_gain, out_weight, channel_gain,
        )
        layer_out = plane_stage(
            second_normed, middle, routes, route_weights,
            expert_gate, expert_up, expert_down, shared_gate, shared_up, shared_down,
        )
        return (layer_out, new_state)
    normed = root_scale(tokens, mix_gain)
    drive_rows = jnp.dot(normed, in_weight, preferred_element_type=jnp.float32).astype(jnp.bfloat16)
    readout, new_state = state_update(
        drive_rows, prior_state, decay_rate, frequency, log_step, input_map, output_map, skip_gain
    )
    activated = jax.nn.gelu(readout).astype(jnp.bfloat16)
    partial_value = jnp.dot(activated, out_weight, preferred_element_type=jnp.float32)
    mixer_out = lax.psum(partial_value.astype(jnp.bfloat16), "tp").astype(jnp.float32)
    middle = (tokens.astype(jnp.float32) + mixer_out).astype(jnp.bfloat16)
    second_normed = root_scale(middle, channel_gain)
    shared_gval = jnp.dot(second_normed, shared_gate, preferred_element_type=jnp.float32)
    shared_uval = jnp.dot(second_normed, shared_up, preferred_element_type=jnp.float32)
    shared_hidden = (jax.nn.silu(shared_gval) * shared_uval).astype(jnp.bfloat16)
    shared_piece = jnp.dot(shared_hidden, shared_down, preferred_element_type=jnp.float32)
    shared_out = lax.psum_scatter(
        shared_piece.astype(jnp.bfloat16), "tp", scatter_dimension=1, tiled=True
    ).astype(jnp.float32)
    half_cols = second_normed.shape[1] // lax.axis_size("tp")
    routed = exchanged_experts(
        second_normed, routes, route_weights, expert_gate, expert_up, expert_down
    )
    own_middle = lax.dynamic_slice_in_dim(middle, lax.axis_index("tp") * half_cols, half_cols, 1)
    layer_out = (own_middle.astype(jnp.float32) + routed + shared_out).astype(jnp.bfloat16)
    return (layer_out, new_state)


def solution(mesh):
    in_specs = (
        P(("grp", "ep"), None),
        P(None, ("grp", "ep"), "tp"),
        P(),
        P(None, "tp"),
        P("tp", None),
        P("tp", None),
        P("tp"),
        P(None, "tp", None, None),
        P(None, "tp", None, None),
        P("tp"),
        P("tp", None),
        P(),
        P("ep", None, "tp"),
        P("ep", None, "tp"),
        P("ep", "tp", None),
        P(None, "tp"),
        P(None, "tp"),
        P("tp", None),
        P(("grp", "ep"), None),
        P(("grp", "ep"), None),
    )
    out_specs = (P(("grp", "ep"), "tp"), P(None, ("grp", "ep"), "tp"))
    return jax.shard_map(body, mesh=mesh, in_specs=in_specs, out_specs=out_specs, check_vma=False)
```
